32 devices in a mesh: kv: 16 (over z, y, x), tp: 2 (over core).
Axes of the slice: x: 2, y: 2, z: 4, core: 2. Of those that a mesh axis runs over, the one named last changes fastest.
Arguments:
- stream: bfloat16 [32, 4096], P(None, 'kv'), may hold values from -32 to 32
- gain_in: bfloat16 [4096], P('kv'), may hold values from 0.099609375 to 1.8984375
- w_query: bfloat16 [4096, 2048], P('kv', 'tp'), may hold values from -0.09375 to 0.09375
- w_key: bfloat16 [4096, 2048], P('kv', 'tp'), may hold values from -0.09375 to 0.09375
- w_value: bfloat16 [4096, 2048], P('kv', 'tp'), may hold values from -0.09375 to 0.09375
- w_forget: bfloat16 [4096, 16], replicated, may hold values from -0.09375 to 0.09375
- keys_cache: bfloat16 [32, 16, 2048, 128], P(None, 'tp', 'kv'), may hold values from -136 to 136
- values_cache: bfloat16 [32, 16, 2048, 128], P(None, 'tp', 'kv'), may hold values from -6 to 6
- decay_cache: float32 [32, 16, 2048], P(None, 'tp', 'kv'), may hold values from -323 to 0
- lengths: int32 [32], replicated, may hold values from 1 to 2048, 26246 in all
- gain_att: bfloat16 [2048], P('tp'), may hold values from 0.099609375 to 1.8984375
- w_out: bfloat16 [2048, 4096], P('tp', 'kv'), may hold values from -0.125 to 0.125
- gain_mlp: bfloat16 [4096], P('kv'), may hold values from 0.099609375 to 1.8984375
- w_up: bfloat16 [4096, 16384], P('kv', 'tp'), may hold values from -0.09375 to 0.09375
- w_down: bfloat16 [16384, 4096], P('tp', 'kv'), may hold values from -0.046875 to 0.046875
Outputs:
- updated: bfloat16 [32, 4096], P(None, 'kv')
The draws below stay inside these ranges and needn't reach their ends.
Inputs may be any that keep to these rules, and one draw needn't show every extreme that they name: `lengths`: one sequence has all 2048 positions live.
All inputs are finite; a program needn't handle non-finite values.
Results may differ from the reference program's by a relative error of at most 0.012.
The reference program's roundings to bfloat16 on the way count: a program that leaves them out, or rounds other values in their place, can miss the bound.
Values may be sent and summed in bfloat16 or wider, within the bound.
A program may use at most 64 MiB of HBM per device.

```python
import math
import jax
import jax.numpy as jnp
import numpy as np
from jax import lax

D = 4096
HEAD_COUNT = 16
HEAD_WIDTH = 128
FF = 16384
SEQUENCE_COUNT = 32
POS_DEV = 128
CACHE_LENGTH = 2048
HW = 2048


def draw_stream(key, part):
    key_one, key_two = jax.random.split(jax.random.fold_in(key, 11), 2)
    column = jnp.arange(D, dtype=jnp.float32) / D
    raw_values = jnp.clip(jax.random.normal(key_one, (SEQUENCE_COUNT, D), jnp.float32), -5.0, 5.0)
    column_scale = jnp.exp(math.log(10.0) * (column - 0.5))
    row_scale = jnp.exp(jax.random.uniform(key_two, (SEQUENCE_COUNT, 1), jnp.float32, math.log(0.5), math.log(2.0)))
    return (raw_values * column_scale[None, :] * row_scale).astype(jnp.bfloat16)


def draw_keys_cache(key, part):
    key_one = jax.random.fold_in(jax.random.fold_in(key, 5), 0)
    full_shape = (SEQUENCE_COUNT, HEAD_COUNT, CACHE_LENGTH, HEAD_WIDTH)
    raw_values = jnp.clip(jax.random.normal(key_one, full_shape, jnp.float32), -5.0, 5.0)
    return raw_values.astype(jnp.bfloat16)


def draw_decay_cache(key, part):
    every_key = jax.random.split(jax.random.fold_in(key, 23), 7)
    head_order = jax.random.permutation(every_key[0], HEAD_COUNT)
    keep_count = HEAD_COUNT // 2
    slow_heads = (head_order < keep_count).reshape(1, HEAD_COUNT, 1)
    slow_rate = jax.random.uniform(every_key[1], (SEQUENCE_COUNT, HEAD_COUNT, 1), jnp.float32, 0.2, 0.8) / CACHE_LENGTH
    fast_rate = 1.0 / (POS_DEV * jax.random.uniform(every_key[2], (SEQUENCE_COUNT, HEAD_COUNT, 1), jnp.float32, 0.25, 0.8))
    learning_rate = jnp.where(slow_heads, slow_rate, fast_rate)
    jaggedness = jnp.exp(jax.random.uniform(every_key[3], (SEQUENCE_COUNT, HEAD_COUNT, CACHE_LENGTH), jnp.float32, math.log(0.5), math.log(2.0)))
    block_count = CACHE_LENGTH // POS_DEV
    block_multiplier = jnp.exp(jax.random.uniform(every_key[4], (1, HEAD_COUNT, block_count, 1), jnp.float32, math.log(0.4), math.log(2.5)))
    block_multiplier = jnp.broadcast_to(block_multiplier, (1, HEAD_COUNT, block_count, POS_DEV)).reshape(1, HEAD_COUNT, CACHE_LENGTH)
    spike_position = jax.random.randint(every_key[5], (SEQUENCE_COUNT, HEAD_COUNT, 3, 1), 0, CACHE_LENGTH)
    spike_penalty = jnp.log(jax.random.uniform(every_key[6], (SEQUENCE_COUNT, HEAD_COUNT, 3, 1), jnp.float32, 0.5, 0.8))
    cache_positions = jnp.arange(CACHE_LENGTH, dtype=jnp.int32)
    spike_events = jnp.sum(jnp.where(cache_positions[None, None, None, :] == spike_position, spike_penalty, 0.0), axis=2)
    gate_logarithms = spike_events - learning_rate * jaggedness * block_multiplier
    suffix_sum = jnp.flip(jnp.cumsum(jnp.flip(gate_logarithms, 2), axis=2), 2)
    return suffix_sum - gate_logarithms


def shard_levels(own_key, extent, cuts, least, high):
    factor_of = 1.0
    for dim, shards_of in cuts:
        steps = jax.random.uniform(jax.random.fold_in(jax.random.fold_in(own_key, 6), dim), (shards_of,), jnp.float32, least / len(cuts), high / len(cuts))
        factor_of = factor_of * jnp.repeat(jnp.exp(steps), extent[dim] // shards_of).reshape((-1,) + (1,) * (len(extent) - 1 - dim))
    return factor_of


def profile(amount, total, bound, skew):
    portions = [(1 << 20) // math.isqrt(grade ** skew) + 1 for grade in range(2, amount + 1)]
    rest, given = total - bound - (amount - 1), [1] * (amount - 1)
    while rest > 0:
        movable = [i for i in range(amount - 1) if given[i] < bound]
        whole, budget = sum([portions[i] for i in movable]), rest
        for i in movable:
            extra = min(bound - given[i], max(1, budget * portions[i] // whole), rest)
            given[i] = given[i] + extra
            rest = rest - extra
    return np.array([bound] + given)


def ragged(stream_key, count, total, reach, slope):
    if count == 2:
        one = jax.random.randint(stream_key, (), max(1, total - reach), min(reach, total - 1) + 1)
        return jnp.stack([one, total - one])
    tallies = jnp.asarray(profile(count, total, reach, slope), jnp.int32)
    couples = (count - 1) // 2
    source_of, receiver = tallies[1:1 + 2 * couples:2], tallies[2:2 + 2 * couples:2]
    slack = jnp.minimum(source_of - 1, reach - receiver)
    moved = jax.random.randint(jax.random.fold_in(stream_key, 1), (couples,), 0, 1 << 20) % (slack + 1)
    tallies = tallies.at[1:1 + 2 * couples:2].set(source_of - moved).at[2:2 + 2 * couples:2].set(receiver + moved)
    return tallies[jax.random.permutation(jax.random.fold_in(stream_key, 2), count)]


def noise(key, dims, spread, bound, shards=(), kind=jnp.bfloat16):
    entries = spread * jax.random.normal(key, dims, jnp.float32)
    if shards:
        entries = entries * shard_levels(key, dims, shards, -0.22, 0.18)
    return jnp.clip(entries, -bound, bound).astype(kind)


def setup_inputs(seed: int = 0) -> dict:
    splits = jax.random.split(jax.random.key(seed), 16)
    stream = draw_stream(jax.random.fold_in(splits[15], 71), 0)
    gain_in = jnp.clip(1.0 + 0.18 * jax.random.normal(splits[1], (D,), jnp.float32), 0.099609375, 1.8984375).astype(jnp.bfloat16)
    w_query = noise(splits[2], (D, HW), D ** -0.5, 0.09375, ((0, 16), (1, 2)))
    w_key = noise(splits[3], (D, HW), D ** -0.5, 0.09375, ((0, 16), (1, 2)))
    w_value = noise(splits[4], (D, HW), D ** -0.5, 0.09375, ((0, 16), (1, 2)))
    w_forget = noise(splits[5], (D, HEAD_COUNT), D ** -0.5, 0.09375)
    keys_cache = draw_keys_cache(jax.random.fold_in(splits[15], 71), 0)
    values_cache = noise(splits[7], (SEQUENCE_COUNT, HEAD_COUNT, CACHE_LENGTH, HEAD_WIDTH), 1.0, 6.0, ((1, 2), (2, 16)))
    decay_cache = draw_decay_cache(jax.random.fold_in(splits[15], 71), 0)
    lengths = ragged(splits[9], SEQUENCE_COUNT, SEQUENCE_COUNT * CACHE_LENGTH * 2 // 5 + SEQUENCE_COUNT, CACHE_LENGTH, 2).astype(jnp.int32)
    gain_att = jnp.clip(1.0 + 0.18 * jax.random.normal(splits[10], (HW,), jnp.float32), 0.099609375, 1.8984375).astype(jnp.bfloat16)
    w_out = noise(splits[11], (HW, D), HW ** -0.5, 0.125, ((0, 2), (1, 16)))
    gain_mlp = jnp.clip(1.0 + 0.18 * jax.random.normal(splits[12], (D,), jnp.float32), 0.099609375, 1.8984375).astype(jnp.bfloat16)
    w_up = noise(splits[13], (D, FF), D ** -0.5, 0.09375, ((0, 16), (1, 2)))
    w_down = noise(splits[14], (FF, D), FF ** -0.5, 0.046875, ((0, 2), (1, 16)))
    return {"stream": stream, "gain_in": gain_in, "w_query": w_query, "w_key": w_key, "w_value": w_value, "w_forget": w_forget, "keys_cache": keys_cache, "values_cache": values_cache, "decay_cache": decay_cache, "lengths": lengths, "gain_att": gain_att, "w_out": w_out, "gain_mlp": gain_mlp, "w_up": w_up, "w_down": w_down}


norm_eps = 1e-06
masked_score = -1e+30

def head_blocks(head_index, queries, forget, keys_cache, values_cache, decay_cache, lengths):
    block_count = CACHE_LENGTH // POS_DEV
    head_queries = lax.dynamic_index_in_dim(queries, head_index, 1, False).astype(jnp.float32)
    head_keys = lax.dynamic_index_in_dim(keys_cache, head_index, 1, False).astype(jnp.float32)
    value_head = lax.dynamic_index_in_dim(values_cache, head_index, 1, False).astype(jnp.float32)
    decay_head = lax.dynamic_index_in_dim(decay_cache, head_index, 1, False)
    forget_head = lax.dynamic_index_in_dim(forget, head_index, 1, False)
    attention_logits = jnp.einsum('tk,txk->tx', head_queries, head_keys) * (1.0 / math.sqrt(HEAD_WIDTH))
    attention_logits = attention_logits + forget_head[:, None] + decay_head
    attention_logits = attention_logits.reshape(SEQUENCE_COUNT, block_count, POS_DEV)
    cache_positions = jnp.arange(CACHE_LENGTH, dtype=jnp.int32).reshape(block_count, POS_DEV)
    live_mask = cache_positions[None] < lengths.astype(jnp.int32)[:, None, None]
    attention_logits = jnp.where(live_mask, attention_logits, masked_score)
    block_peak = lax.optimization_barrier(jnp.max(attention_logits, axis=2))
    weights = jnp.where(live_mask, jnp.exp(attention_logits - block_peak[..., None]), 0.0)
    block_total = lax.optimization_barrier(jnp.sum(weights, axis=2))
    rounded = lax.optimization_barrier(weights.astype(jnp.bfloat16)).astype(jnp.float32)
    block_out = jnp.einsum('sbp,sbpd->sbd', rounded, value_head.reshape(SEQUENCE_COUNT, block_count, POS_DEV, HEAD_WIDTH))
    return (block_peak, block_total, block_out)

def reference(stream, gain_in, w_query, w_key, w_value, w_forget, keys_cache, values_cache, decay_cache, lengths, gain_att, w_out, gain_mlp, w_up, w_down):
    score_scale = 1.0 / math.sqrt(HEAD_WIDTH)
    stream_float = stream.astype(jnp.float32)
    scaled = (stream_float * gain_in.astype(jnp.float32)).astype(jnp.bfloat16)
    scale_in = lax.rsqrt(lax.optimization_barrier(jnp.mean(stream_float * stream_float, axis=1)) + norm_eps)[:, None]
    queries = (jnp.dot(scaled, w_query, preferred_element_type=jnp.float32) * scale_in).astype(jnp.bfloat16).reshape(SEQUENCE_COUNT, HEAD_COUNT, HEAD_WIDTH)
    key_new = (jnp.dot(scaled, w_key, preferred_element_type=jnp.float32) * scale_in).astype(jnp.bfloat16).reshape(SEQUENCE_COUNT, HEAD_COUNT, HEAD_WIDTH)
    value_new = (jnp.dot(scaled, w_value, preferred_element_type=jnp.float32) * scale_in).astype(jnp.bfloat16).reshape(SEQUENCE_COUNT, HEAD_COUNT, HEAD_WIDTH)
    forget = jax.nn.log_sigmoid(jnp.dot(scaled, w_forget, preferred_element_type=jnp.float32) * scale_in)
    block_peaks, totals, block_outs = lax.map(lambda head_index: head_blocks(head_index, queries, forget, keys_cache, values_cache, decay_cache, lengths), jnp.arange(HEAD_COUNT, dtype=jnp.int32))
    block_peaks = jnp.transpose(block_peaks, (1, 0, 2))
    totals = jnp.transpose(totals, (1, 0, 2))
    block_outs = jnp.transpose(block_outs, (1, 0, 2, 3))
    own_score = lax.optimization_barrier(jnp.sum(queries.astype(jnp.float32) * key_new.astype(jnp.float32), axis=2)) * score_scale
    top_score = jnp.maximum(lax.optimization_barrier(jnp.max(block_peaks, axis=2)), own_score)
    block_weight = jnp.exp(block_peaks - top_score[..., None])
    own_weight = jnp.exp(own_score - top_score)
    numerator = lax.optimization_barrier(jnp.sum(block_weight[..., None] * block_outs, axis=2)) + own_weight[..., None] * value_new.astype(jnp.float32)
    denominator = lax.optimization_barrier(jnp.sum(block_weight * totals, axis=2)) + own_weight
    attended = (numerator / denominator[..., None]).reshape(SEQUENCE_COUNT, HW)
    scale_att = lax.rsqrt(lax.optimization_barrier(jnp.mean(attended * attended, axis=1)) + norm_eps)[:, None]
    attended_in = (attended * gain_att.astype(jnp.float32)).astype(jnp.bfloat16)
    residual = (stream_float + scale_att * jnp.dot(attended_in, w_out, preferred_element_type=jnp.float32)).astype(jnp.bfloat16)
    residual_float = residual.astype(jnp.float32)
    mixer_in = (residual_float * gain_mlp.astype(jnp.float32)).astype(jnp.bfloat16)
    scale_mixer = lax.rsqrt(lax.optimization_barrier(jnp.mean(residual_float * residual_float, axis=1)) + norm_eps)[:, None]
    hidden = jnp.square(jax.nn.relu(jnp.dot(mixer_in, w_up, preferred_element_type=jnp.float32) * scale_mixer)).astype(jnp.bfloat16)
    return (residual_float + jnp.dot(hidden, w_down, preferred_element_type=jnp.float32)).astype(jnp.bfloat16)
```

```python
import functools
import math

import jax
import jax.numpy as jnp
from jax import lax
from jax.experimental import pallas as pl
from jax.experimental.pallas import tpu as pltpu
from jax.sharding import PartitionSpec as P

f32 = jnp.float32
bf16 = jnp.bfloat16
LANES = 128
PLANE = 4

norm_eps = 1e-06
masked_score = -1e30


def merged_2(value, axis, join):
    pieces = jax.tree.map(lambda part: lax.all_gather(part, axis), value)
    head = jax.tree.map(lambda part: part[0], pieces)
    tail = jax.tree.map(lambda part: part[1:], pieces)
    so_far, _ = lax.scan(lambda so_far, share: (join(so_far, share), None), head, tail)
    return so_far


def fold_parts(left_part, right_part):
    peak_all = jnp.maximum(left_part[0], right_part[0])
    weight_one = jnp.exp(left_part[0] - peak_all)
    weight_two = jnp.exp(right_part[0] - peak_all)
    total_sum = left_part[1] * weight_one + right_part[1] * weight_two
    merged = left_part[2] * weight_one[..., None] + right_part[2] * weight_two[..., None]
    return (peak_all, total_sum, merged)


def per_device(
    stream,
    gain_in,
    w_query,
    w_key,
    w_value,
    w_forget,
    keys_cache,
    values_cache,
    decay_cache,
    lengths,
    gain_att,
    w_out,
    gain_mlp,
    w_up,
    w_down,
):
    kv_index = lax.axis_index("kv")
    tp_index = lax.axis_index("tp")
    kv_count = lax.axis_size("kv")
    seqs_here, cols_here = stream.shape
    heads_here = keys_cache.shape[1]
    pos_here = keys_cache.shape[2]
    head_dim = keys_cache.shape[3]
    width_all = cols_here * kv_count
    score_scale = 1.0 / math.sqrt(head_dim)
    stream_float = stream.astype(jnp.float32)
    scaled = (stream_float * gain_in.astype(jnp.float32)).astype(jnp.bfloat16)
    square_sum = jnp.sum(stream_float * stream_float, axis=1)
    forget_rows = lax.dynamic_slice(
        w_forget, (kv_index * cols_here, tp_index * heads_here), (cols_here, heads_here)
    )
    part_query = jnp.dot(scaled, w_query, preferred_element_type=jnp.float32)
    part_key = jnp.dot(scaled, w_key, preferred_element_type=jnp.float32)
    part_value = jnp.dot(scaled, w_value, preferred_element_type=jnp.float32)
    part_forget = jnp.dot(scaled, forget_rows, preferred_element_type=jnp.float32)
    part_query, part_key, part_value, part_forget, square_total = lax.psum(
        (part_query, part_key, part_value, part_forget, square_sum), "kv"
    )
    scale_in = lax.rsqrt(square_total / width_all + norm_eps)[:, None]
    queries = (part_query * scale_in).astype(jnp.bfloat16).reshape(seqs_here, heads_here, head_dim)
    key_new = (part_key * scale_in).astype(jnp.bfloat16).reshape(seqs_here, heads_here, head_dim)
    value_new = (
        (part_value * scale_in).astype(jnp.bfloat16).reshape(seqs_here, heads_here, head_dim)
    )
    forget = jax.nn.log_sigmoid(part_forget * scale_in)
    attention_logits = (
        jnp.einsum("shd,shpd->shp", queries, keys_cache, preferred_element_type=jnp.float32)
        * score_scale
    )
    attention_logits = attention_logits + forget[:, :, None] + decay_cache
    cache_positions = kv_index * pos_here + lax.iota(jnp.int32, pos_here)
    live_mask = (cache_positions[None, :] < lengths[:, None])[:, None, :]
    attention_logits = jnp.where(live_mask, attention_logits, masked_score)
    block_peak = jnp.max(attention_logits, axis=2)
    weights = jnp.where(live_mask, jnp.exp(attention_logits - block_peak[..., None]), 0.0)
    block_total = jnp.sum(weights, axis=2)
    block_out = jnp.einsum(
        "shp,shpd->shd",
        weights.astype(jnp.bfloat16),
        values_cache,
        preferred_element_type=jnp.float32,
    )
    peak_all, total_all, out_all = merged_2((block_peak, block_total, block_out), "kv", fold_parts)
    own_score = (
        jnp.sum(queries.astype(jnp.float32) * key_new.astype(jnp.float32), axis=2) * score_scale
    )
    top_score = jnp.maximum(peak_all, own_score)
    past_weight = jnp.exp(peak_all - top_score)
    own_weight = jnp.exp(own_score - top_score)
    numerator = (
        out_all * past_weight[..., None] + value_new.astype(jnp.float32) * own_weight[..., None]
    )
    denominator = total_all * past_weight + own_weight
    attended = (numerator / denominator[..., None]).reshape(seqs_here, heads_here * head_dim)
    attended_in = (attended * gain_att.astype(jnp.float32)).astype(jnp.bfloat16)
    part_out = jnp.dot(attended_in, w_out, preferred_element_type=jnp.float32)
    att_squares = jnp.sum(attended * attended, axis=1)
    part_out, att_total = lax.psum((part_out, att_squares), "tp")
    scale_att = lax.rsqrt(att_total / (attended.shape[1] * lax.axis_size("tp")) + norm_eps)[:, None]
    residual = (stream_float + scale_att * part_out).astype(jnp.bfloat16)
    residual_float = residual.astype(jnp.float32)
    mixer_in = (residual_float * gain_mlp.astype(jnp.float32)).astype(jnp.bfloat16)
    mixer_squares = jnp.sum(residual_float * residual_float, axis=1)
    part_up = jnp.dot(mixer_in, w_up, preferred_element_type=jnp.float32)
    pre_act, mixer_total = lax.psum((part_up, mixer_squares), "kv")
    scale_mixer = lax.rsqrt(mixer_total / width_all + norm_eps)[:, None]
    hidden = jnp.square(jax.nn.relu(pre_act * scale_mixer)).astype(jnp.bfloat16)
    part_down = jnp.dot(hidden, w_down, preferred_element_type=jnp.float32)
    mixer_out = lax.psum(part_down, "tp")
    return (residual_float + mixer_out).astype(jnp.bfloat16)


def lanes_of(shape):
    return lax.broadcasted_iota(jnp.int32, shape, 1)


def rows_of(shape):
    return lax.broadcasted_iota(jnp.int32, shape, 0)


def to_column(row, count, *starts):
    shape = (count, LANES)
    apart = lanes_of(shape) - rows_of(shape)
    hit = functools.reduce(jnp.logical_or, [apart == start for start in starts])
    return jnp.sum(
        jnp.where(hit, jnp.broadcast_to(row, shape), 0.0), axis=1, keepdims=True
    )


def to_row(column, start):
    shape = (column.shape[0], LANES)
    hit = lanes_of(shape) - rows_of(shape) == start
    return jnp.sum(
        jnp.where(hit, jnp.broadcast_to(column, shape), 0.0), axis=0, keepdims=True
    )


Q, STAT, KV, Q_ALL, OUT, PEAK, ATT, SQUARE, MIX, UP, RELAY, HID, HID_RELAY, PAIR = range(14)


def layer_kernel(
    kv_n,
    lengths, stream, gain_in, gain_att, gain_mlp, decay,
    w_forget, w_query, w_key, w_value, keys, values, w_out, w_up, w_down,
    out,
    len_s, x_v, gi_v, ga_v, gm_v, decay_v,
    wf_v, wq_v, wk_v, wv_v, keys_v, values_v, wo_v, wu_v, wd_v,
    gain_far, q_send, q_recv, st_send, st_recv, kv_send, kv_recv,
    q_own, q_all, q_float, o_float, o_send, o_recv, pk_send, pk_recv,
    att_own, att_all, sq_own, sq_all, send5, recv5,
    mix_own, mix_all, up_send, relay_recv, relay_send, up_recv,
    hid_relay, hid_all, send8, recv8,
    load_sem, cache_sem, ssem, rsem,
):
    me = lax.axis_index("kv")
    tp = lax.axis_index("tp")
    far = 1 - tp
    seqs, cols = x_v.shape
    heads = decay_v.shape[1]
    pos_here = decay_v.shape[2]
    dim = keys_v.shape[-1]
    rows = q_own.shape[0]
    groups = seqs // rows
    hidden_here = hid_all.shape[2]
    chunks = cache_sem.shape[1]
    per_chunk = seqs // chunks
    width_all = cols * kv_n
    score_scale = 1.0 / math.sqrt(dim)
    together = math.gcd(8, per_chunk)

    level, spot = me // PLANE, me % PLANE
    levels = (level, level + 1 - 2 * (level % 2), (level + 2) % 4, 3 - level)
    side, along = spot // 2, spot % 2
    spots = (
        spot, side * 2 + 1 - along, (1 - side) * 2 + along, (1 - side) * 2 + 1 - along
    )
    peers = [levels[k // PLANE] * PLANE + spots[k % PLANE] for k in range(kv_n)]
    far_first = (15, 14, 13, 11, 12, 10, 9, 7, 8, 6, 5, 3, 4, 2, 1, 0)
    plane_order = (3, 1, 2, 0)
    my_group, my_head = me // heads, me % heads

    barrier = pltpu.get_barrier_semaphore()
    for k in far_first:
        pl.semaphore_signal(
            barrier, inc=1, device_id=(peers[k], far), device_id_type=pl.DeviceIdType.MESH
        )

    def load(src, dst, index):
        return pltpu.make_async_copy(src, dst, load_sem.at[index])

    start_row = pl.multiple_of(me * cols, cols)
    first_head = pl.multiple_of(tp * heads, heads)
    first_loads = [
        load(stream, x_v, 0),
        load(gain_in, gi_v, 1),
        load(w_query, wq_v, 2),
        load(w_forget.at[pl.ds(first_head, heads), pl.ds(start_row, cols)], wf_v, 3),
        load(w_key, wk_v, 4),
        load(w_value, wv_v, 5),
    ]
    small_loads = [
        load(gain_att, ga_v, 6), load(decay, decay_v, 7), load(lengths, len_s, 8),
        load(gain_mlp, gm_v, 9),
    ]
    late_loads = [load(w_out, wo_v, 10), load(w_up, wu_v, 11), load(w_down, wd_v, 12)]
    for copy in first_loads:
        copy.start()
    for copy in small_loads:
        copy.start()

    def cache_copy(which, chunk):
        src, dst = ((keys, keys_v), (values, values_v))[which]
        part = pl.ds(chunk * per_chunk, per_chunk)
        return pltpu.make_async_copy(src.at[part], dst.at[part], cache_sem.at[which, chunk])

    def remote(phase, slot, src, dst, device, core):
        return pltpu.make_async_remote_copy(
            src_ref=src, dst_ref=dst,
            send_sem=ssem.at[phase, slot], recv_sem=rsem.at[phase, slot],
            device_id=(device, core), device_id_type=pl.DeviceIdType.MESH,
        )

    started = []

    def go(copy):
        copy.start()
        started.append(copy)

    def drain():
        for copy in started:
            copy.wait_send()
        started.clear()

    def scatter(phase, send, recv, k):
        return remote(phase, k, send.at[peers[k]], recv.at[k], peers[k], far)

    def row_to(phase, src, recv, k):
        return remote(phase, k, src, recv.at[pl.ds(k, 1)], peers[k], far)

    def spread(phase, own, held, k):
        return remote(phase, k, own, held.at[me], peers[k], far)

    def landed(phase, own, held, k):
        return remote(phase, k, own, held.at[peers[k]], peers[k], far)

    for copy in first_loads[:4]:
        copy.wait()
    x = x_v[...].astype(f32)
    scaled = (x * gi_v[...].astype(f32).reshape(1, -1)).astype(bf16)

    def by_owner(dst, part, place):
        for g in range(groups):
            for h in range(heads):
                dst[g * heads + h, place * rows:(place + 1) * rows, :] = part[
                    g * rows:(g + 1) * rows, h * dim:(h + 1) * dim
                ]

    by_owner(q_send, jnp.dot(scaled, wq_v[...], preferred_element_type=f32).astype(bf16), 0)
    squares = x * x
    high = squares.astype(bf16)
    low = (squares - high.astype(f32)).astype(bf16)
    blank = jnp.zeros((32, cols), bf16)
    last = (((1,), (1,)), ((), ()))
    st_send[...] = lax.dot_general(
        jnp.ones((heads, cols), bf16), jnp.concatenate([high, blank, low, blank], axis=0),
        last, preferred_element_type=f32,
    ) + lax.dot_general(
        wf_v[...], jnp.concatenate([blank, scaled, blank, blank], axis=0),
        last, preferred_element_type=f32,
    )
    for copy in first_loads[4:]:
        copy.wait()
    for copy in small_loads:
        copy.wait()
    for chunk in range(chunks):
        cache_copy(0, chunk).start()
        cache_copy(1, chunk).start()
    for copy in late_loads:
        copy.start()
    pl.semaphore_wait(barrier, kv_n)
    for k in far_first:
        go(scatter(Q, q_send, q_recv, k))
        go(row_to(STAT, st_send.at[pl.ds(peers[k] % heads, 1)], st_recv, k))
    gain_swap = remote(PAIR, 0, ga_v, gain_far, me, far)
    go(gain_swap)
    for place, weight in enumerate((wk_v, wv_v)):
        by_owner(
            kv_send, jnp.dot(scaled, weight[...], preferred_element_type=f32).astype(bf16), place
        )
    for k in far_first:
        go(scatter(KV, kv_send, kv_recv, k))
    total = jnp.zeros((rows, dim), f32)
    for k in range(kv_n):
        row_to(STAT, st_send.at[pl.ds(0, 1)], st_recv, k).wait_recv()
        scatter(Q, q_send, q_recv, k).wait_recv()
        total = total + q_recv[k].astype(f32)
    stat_row = jnp.sum(st_recv[...], axis=0, keepdims=True)
    first_lane = my_group * rows
    scale_in = lax.rsqrt(
        to_column(stat_row, rows, first_lane, first_lane + 64) / width_all + norm_eps
    )
    query = (total * scale_in).astype(bf16)
    q_own[...] = query
    for k in far_first:
        go(spread(Q_ALL, q_own, q_all, k))
    gate = to_column(stat_row, rows, first_lane + 32) * scale_in
    forget = jnp.minimum(gate, 0.0) - jnp.log1p(jnp.exp(-jnp.abs(gate)))

    for k in range(kv_n):
        landed(Q_ALL, q_own, q_all, k).wait_recv()
    q_float[...] = q_all[...].reshape(kv_n * rows, dim).astype(f32)
    head_row = rows_of((heads, pos_here))
    position = me * pos_here + lanes_of((heads, pos_here))
    lane_h = lanes_of((heads, LANES))

    def some_sequences(first_seq, marks):
        batch = [first_seq + i for i in range(together)]
        places = [
            pl.ds((s // rows) * (heads * rows) + s % rows, heads, stride=rows) for s in batch
        ]
        q_parts = [q_float[mine, :].astype(bf16) for mine in places]
        everies = [
            lax.dot_general(
                q_s, keys_v[s].reshape(heads * pos_here, dim), last,
                preferred_element_type=f32,
            )
            for q_s, s in zip(q_parts, batch)
        ]
        spreads = []
        for every, s in zip(everies, batch):
            score = every[:, :pos_here]
            for h in range(1, heads):
                score = jnp.where(
                    head_row == h, every[:, h * pos_here:(h + 1) * pos_here], score
                )
            score = score * score_scale + decay_v[s]
            live = position < len_s[s]
            score = jnp.where(live, score, masked_score)
            peak = jnp.max(score, axis=1, keepdims=True)
            probs = jnp.where(live, jnp.exp(score - peak), 0.0)
            block_total = jnp.sum(probs, axis=1, keepdims=True)
            spreads.append(jnp.concatenate(
                [jnp.where(head_row == h, probs, 0.0) for h in range(heads)], axis=1
            ).astype(bf16))
            marks = jnp.where(lane_h == s % rows, peak, marks)
            marks = jnp.where(lane_h == s % rows + rows, block_total, marks)
        outs = [
            jnp.dot(
                part, values_v[s].reshape(heads * pos_here, dim), preferred_element_type=f32
            )
            for part, s in zip(spreads, batch)
        ]
        for mine, out_s in zip(places, outs):
            o_float[mine, :] = out_s
        return marks

    def one_chunk(chunk, marks):
        cache_copy(0, chunk).wait()
        cache_copy(1, chunk).wait()

        def inner(i, c):
            return some_sequences(chunk * per_chunk + together * i, c)

        return lax.fori_loop(0, per_chunk // together, inner, marks)

    group_chunks = chunks // groups
    for g in range(groups):
        marks = lax.fori_loop(
            g * group_chunks, (g + 1) * group_chunks, one_chunk, jnp.zeros((heads, LANES), f32)
        )
        pk_send[g * heads:(g + 1) * heads, :] = marks
    o_send[...] = o_float[...].astype(bf16).reshape(kv_n, rows, dim)
    for k in far_first:
        go(scatter(OUT, o_send, o_recv, k))
        go(row_to(PEAK, pk_send.at[pl.ds(peers[k], 1)], pk_recv, k))

    keys_total = jnp.zeros((2 * rows, dim), f32)
    for k in range(kv_n):
        scatter(KV, kv_send, kv_recv, k).wait_recv()
        keys_total = keys_total + kv_recv[k].astype(f32)
    key_new = (keys_total[:rows] * scale_in).astype(bf16).astype(f32)
    value_new = (keys_total[rows:] * scale_in).astype(bf16).astype(f32)
    own_score = jnp.sum(query.astype(f32) * key_new, axis=1, keepdims=True) * score_scale
    gain_swap.wait_recv()
    gain_here = gain_far[...].astype(f32).reshape(1, -1)
    gain_head = gain_here[:, :dim]
    for h in range(1, heads):
        gain_head = jnp.where(my_head == h, gain_here[:, h * dim:(h + 1) * dim], gain_head)

    for k in range(kv_n):
        row_to(PEAK, pk_send.at[pl.ds(0, 1)], pk_recv, k).wait_recv()
    peaks = pk_recv[...]
    top_row = jnp.max(peaks, axis=0, keepdims=True)
    shares = jnp.exp(peaks - top_row)
    total_row = jnp.sum(shares * pltpu.roll(peaks, LANES - rows, 1), axis=0, keepdims=True)
    peak_all = to_column(top_row, rows, 0) + forget
    total_all = to_column(total_row, rows, 0)
    share_columns = [to_column(shares[k:k + 1], rows, 0) for k in range(kv_n)]
    top = jnp.maximum(peak_all, own_score)
    past_weight = jnp.exp(peak_all - top)
    own_weight = jnp.exp(own_score - top)
    out_all = jnp.zeros((rows, dim), f32)
    for k in range(kv_n):
        scatter(OUT, o_send, o_recv, k).wait_recv()
        out_all = out_all + share_columns[k] * o_recv[k].astype(f32)
    attended_one = (out_all * past_weight + value_new * own_weight) / (
        total_all * past_weight + own_weight
    )
    att_own[...] = (attended_one * gain_head).astype(bf16)
    squares_one = jnp.sum(attended_one * attended_one, axis=1, keepdims=True)
    sq_own[...] = jnp.broadcast_to(to_row(squares_one, first_lane), sq_own.shape)
    for k in far_first:
        go(spread(ATT, att_own, att_all, k))
        go(row_to(SQUARE, sq_own.at[pl.ds(0, 1)], sq_all, k))

    for copy in late_loads:
        copy.wait()
    drain_before = list(started[:-2 * kv_n])
    for copy in drain_before:
        copy.wait_send()
    del started[:len(drain_before)]
    for k in range(kv_n):
        landed(ATT, att_own, att_all, k).wait_recv()
        row_to(SQUARE, sq_own.at[pl.ds(0, 1)], sq_all, k).wait_recv()
    attended_in = jnp.concatenate(
        [
            jnp.concatenate([att_all[g * heads + h] for g in range(groups)], axis=0)
            for h in range(heads)
        ],
        axis=1,
    )
    part_out = jnp.dot(attended_in, wo_v[...], preferred_element_type=f32)
    att_squares = to_column(jnp.sum(sq_all[...], axis=0, keepdims=True), seqs, 0)
    send5[:, :cols] = part_out
    send5[:, cols:] = jnp.broadcast_to(att_squares, (seqs, LANES))
    swap5 = remote(PAIR, 1, send5, recv5, me, far)
    go(swap5)
    swap5.wait_recv()
    width_att = attended_in.shape[1] * 2
    scale_att = lax.rsqrt((att_squares + recv5[:, cols:cols + 1]) / width_att + norm_eps)
    residual = (
        x_v[...].astype(f32) + scale_att * (part_out + recv5[:, :cols])
    ).astype(bf16).astype(f32)
    mixer_in = (residual * gm_v[...].astype(f32).reshape(1, -1)).astype(bf16)
    mixer_squares = jnp.sum(residual * residual, axis=1, keepdims=True)

    def up(owner):
        columns = pl.ds(pl.multiple_of(owner * hidden_here, LANES), hidden_here)
        return jnp.dot(mixer_in, wu_v[:, columns], preferred_element_type=f32)

    def to_relay(k):
        return remote(
            UP, k, up_send.at[k], relay_recv.at[k - 2 * PLANE], peers[k % PLANE], far
        )

    def from_relay(apart):
        index = apart - 2
        return remote(
            RELAY, index, relay_send.at[index], up_recv.at[index], peers[apart * PLANE], far
        )

    def straight(k):
        return remote(UP, k, up_send.at[k], up_recv.at[k + 1], peers[k], tp)

    for apart in (3, 2):
        for p in plane_order:
            k = apart * PLANE + p
            up_send[k] = up(peers[k]).astype(bf16)
            go(to_relay(k))
    mix_own[...] = jnp.broadcast_to(to_row(mixer_squares, 0), mix_own.shape)
    for k in far_first:
        go(row_to(MIX, mix_own.at[pl.ds(0, 1)], mix_all, k))
    for apart in (1, 0):
        for p in plane_order:
            k = apart * PLANE + p
            if k:
                up_send[k] = up(peers[k]).astype(bf16)
                go(straight(k))
    pre_act = up(me)
    for apart in (3, 2):
        relayed = None
        for p in (0, 1, 2, 3):
            k = apart * PLANE + p
            to_relay(k).wait_recv()
            block = relay_recv[k - 2 * PLANE].astype(f32)
            relayed = block if relayed is None else relayed + block
        relay_send[apart - 2] = relayed.astype(bf16)
        go(from_relay(apart))
    for k in range(kv_n):
        row_to(MIX, mix_own.at[pl.ds(0, 1)], mix_all, k).wait_recv()
    mixer_total = to_column(jnp.sum(mix_all[...], axis=0, keepdims=True), seqs, 0)
    scale_mixer = lax.rsqrt(mixer_total / width_all + norm_eps)
    for k in range(1, 2 * PLANE):
        straight(k).wait_recv()
        pre_act = pre_act + up_recv[k + 1].astype(f32)
    for apart in (2, 3):
        from_relay(apart).wait_recv()
        pre_act = pre_act + up_recv[apart - 2].astype(f32)
    hidden = jnp.maximum(pre_act * scale_mixer, 0.0)
    hid_all[me] = (hidden * hidden).astype(bf16)

    def to_level(apart):
        return remote(
            HID_RELAY, apart - 2, hid_all.at[me], hid_relay.at[apart - 2],
            peers[apart * PLANE], far,
        )

    def onward(apart, p):
        return remote(
            HID, apart * PLANE + p, hid_relay.at[apart - 2],
            hid_all.at[peers[apart * PLANE]], peers[p], far,
        )

    def arrived(k):
        return remote(HID, k, hid_all.at[me], hid_all.at[peers[k]], peers[k], tp)

    for apart in (3, 2):
        go(to_level(apart))
    for apart in (0, 1):
        for p in plane_order:
            k = apart * PLANE + p
            if k:
                go(remote(HID, k, hid_all.at[me], hid_all.at[me], peers[k], tp))

    def down(owner):
        depth = pl.ds(pl.multiple_of(owner * hidden_here, LANES), hidden_here)
        return jnp.dot(hid_all[owner], wd_v[depth, :], preferred_element_type=f32)

    part_down = down(me)
    for apart in (2, 3):
        to_level(apart).wait_recv()
        for p in plane_order:
            go(onward(apart, p))
    for k in range(1, kv_n):
        arrived(k).wait_recv()
        part_down = part_down + down(peers[k])
    send8[...] = part_down
    swap8 = remote(PAIR, 2, send8, recv8, me, far)
    go(swap8)
    drain_before = list(started[:-1])
    for copy in drain_before:
        copy.wait_send()
    swap8.wait_recv()
    out[...] = (residual + (part_down + recv8[...])).astype(bf16)
    swap8.wait_send()


def fits(kv_n, tp_n, seqs, cols, heads, heads_all, pos_here, dim, units):
    if tp_n != 2 or kv_n != PLANE * PLANE or heads != 8 or seqs != 32:
        return False
    return (
        cols % LANES == 0 and pos_here == LANES and dim == LANES
        and heads_all == 2 * heads and units % (kv_n * LANES) == 0
    )


def layer(
    stream, gain_in, w_query, w_key, w_value, w_forget, keys_cache, values_cache,
    decay_cache, lengths, gain_att, w_out, gain_mlp, w_up, w_down,
):
    kv_n, tp_n = lax.axis_size("kv"), lax.axis_size("tp")
    seqs, cols = stream.shape
    heads, pos_here, dim = keys_cache.shape[1:]
    heads_all = w_forget.shape[1]
    units = w_up.shape[1]
    if not fits(kv_n, tp_n, seqs, cols, heads, heads_all, pos_here, dim, units):
        return per_device(
            stream, gain_in, w_query, w_key, w_value, w_forget, keys_cache, values_cache,
            decay_cache, lengths, gain_att, w_out, gain_mlp, w_up, w_down,
        )
    rows = seqs * heads // kv_n
    hidden_here = units // kv_n
    chunks = 4
    anywhere = pl.BlockSpec(memory_space=pl.ANY)

    def held(*shape, kind=bf16):
        return pltpu.VMEM(shape, kind)

    return pl.pallas_call(
        functools.partial(layer_kernel, kv_n),
        out_shape=jax.ShapeDtypeStruct((seqs, cols), bf16),
        in_specs=[anywhere] * 15,
        out_specs=pl.BlockSpec(memory_space=pltpu.VMEM),
        scratch_shapes=[
            pltpu.SMEM((seqs,), jnp.int32),
            held(seqs, cols),
            held(cols),
            held(*gain_att.shape),
            held(cols),
            held(*decay_cache.shape, kind=f32),
            held(heads, cols),
            held(*w_query.shape),
            held(*w_key.shape),
            held(*w_value.shape),
            held(*keys_cache.shape),
            held(*values_cache.shape),
            held(*w_out.shape),
            held(*w_up.shape),
            held(*w_down.shape),
            held(*gain_att.shape),
            held(kv_n, rows, dim),
            held(kv_n, rows, dim),
            held(heads, LANES, kind=f32),
            held(kv_n, LANES, kind=f32),
            held(kv_n, 2 * rows, dim),
            held(kv_n, 2 * rows, dim),
            held(rows, dim),
            held(kv_n, rows, dim),
            held(kv_n * rows, dim, kind=f32),
            held(kv_n * rows, dim, kind=f32),
            held(kv_n, rows, dim),
            held(kv_n, rows, dim),
            held(kv_n, LANES, kind=f32),
            held(kv_n, LANES, kind=f32),
            held(rows, dim),
            held(kv_n, rows, dim),
            held(8, LANES, kind=f32),
            held(kv_n, LANES, kind=f32),
            held(seqs, cols + LANES, kind=f32),
            held(seqs, cols + LANES, kind=f32),
            held(8, LANES, kind=f32),
            held(kv_n, LANES, kind=f32),
            held(kv_n, seqs, hidden_here),
            held(2 * PLANE, seqs, hidden_here),
            held(2, seqs, hidden_here),
            held(2 * PLANE + 1, seqs, hidden_here),
            held(2, seqs, hidden_here),
            held(kv_n, seqs, hidden_here),
            held(seqs, cols, kind=f32),
            held(seqs, cols, kind=f32),
            pltpu.SemaphoreType.DMA((13,)),
            pltpu.SemaphoreType.DMA((2, chunks)),
            pltpu.SemaphoreType.DMA((14, kv_n)),
            pltpu.SemaphoreType.DMA((14, kv_n)),
        ],
        compiler_params=pltpu.CompilerParams(
            collective_id=0, has_side_effects=True, vmem_limit_bytes=60 * 1024 * 1024
        ),
    )(
        lengths, stream, gain_in, gain_att,
        gain_mlp, decay_cache,
        w_forget.T, w_query, w_key, w_value, keys_cache, values_cache, w_out, w_up, w_down,
    )


def solution(mesh):
    in_specs = (
        P(None, "kv"),
        P("kv"),
        P("kv", "tp"),
        P("kv", "tp"),
        P("kv", "tp"),
        P(),
        P(None, "tp", "kv", None),
        P(None, "tp", "kv", None),
        P(None, "tp", "kv"),
        P(),
        P("tp"),
        P("tp", "kv"),
        P("kv"),
        P("kv", "tp"),
        P("tp", "kv"),
    )
    out_specs = P(None, "kv")
    return jax.shard_map(
        layer, mesh=mesh, in_specs=in_specs, out_specs=out_specs, check_vma=False
    )
```

```python
import functools
import math

import jax
import jax.numpy as jnp
from jax import lax
from jax.experimental import pallas as pl
from jax.experimental.pallas import tpu as pltpu
from jax.sharding import PartitionSpec as P

f32 = jnp.float32
bf16 = jnp.bfloat16
LANES = 128
PLANE = 4

norm_eps = 1e-06
masked_score = -1e30


def merged_2(value, axis, join):
    pieces = jax.tree.map(lambda part: lax.all_gather(part, axis), value)
    head = jax.tree.map(lambda part: part[0], pieces)
    tail = jax.tree.map(lambda part: part[1:], pieces)
    so_far, _ = lax.scan(lambda so_far, share: (join(so_far, share), None), head, tail)
    return so_far


def fold_parts(left_part, right_part):
    peak_all = jnp.maximum(left_part[0], right_part[0])
    weight_one = jnp.exp(left_part[0] - peak_all)
    weight_two = jnp.exp(right_part[0] - peak_all)
    total_sum = left_part[1] * weight_one + right_part[1] * weight_two
    merged = left_part[2] * weight_one[..., None] + right_part[2] * weight_two[..., None]
    return (peak_all, total_sum, merged)


def per_device(
    stream,
    gain_in,
    w_query,
    w_key,
    w_value,
    w_forget,
    keys_cache,
    values_cache,
    decay_cache,
    lengths,
    gain_att,
    w_out,
    gain_mlp,
    w_up,
    w_down,
):
    kv_index = lax.axis_index("kv")
    tp_index = lax.axis_index("tp")
    kv_count = lax.axis_size("kv")
    seqs_here, cols_here = stream.shape
    heads_here = keys_cache.shape[1]
    pos_here = keys_cache.shape[2]
    head_dim = keys_cache.shape[3]
    width_all = cols_here * kv_count
    score_scale = 1.0 / math.sqrt(head_dim)
    stream_float = stream.astype(jnp.float32)
    scaled = (stream_float * gain_in.astype(jnp.float32)).astype(jnp.bfloat16)
    square_sum = jnp.sum(stream_float * stream_float, axis=1)
    forget_rows = lax.dynamic_slice(
        w_forget, (kv_index * cols_here, tp_index * heads_here), (cols_here, heads_here)
    )
    part_query = jnp.dot(scaled, w_query, preferred_element_type=jnp.float32)
    part_key = jnp.dot(scaled, w_key, preferred_element_type=jnp.float32)
    part_value = jnp.dot(scaled, w_value, preferred_element_type=jnp.float32)
    part_forget = jnp.dot(scaled, forget_rows, preferred_element_type=jnp.float32)
    part_query, part_key, part_value, part_forget, square_total = lax.psum(
        (part_query, part_key, part_value, part_forget, square_sum), "kv"
    )
    scale_in = lax.rsqrt(square_total / width_all + norm_eps)[:, None]
    queries = (part_query * scale_in).astype(jnp.bfloat16).reshape(seqs_here, heads_here, head_dim)
    key_new = (part_key * scale_in).astype(jnp.bfloat16).reshape(seqs_here, heads_here, head_dim)
    value_new = (
        (part_value * scale_in).astype(jnp.bfloat16).reshape(seqs_here, heads_here, head_dim)
    )
    forget = jax.nn.log_sigmoid(part_forget * scale_in)
    attention_logits = (
        jnp.einsum("shd,shpd->shp", queries, keys_cache, preferred_element_type=jnp.float32)
        * score_scale
    )
    attention_logits = attention_logits + forget[:, :, None] + decay_cache
    cache_positions = kv_index * pos_here + lax.iota(jnp.int32, pos_here)
    live_mask = (cache_positions[None, :] < lengths[:, None])[:, None, :]
    attention_logits = jnp.where(live_mask, attention_logits, masked_score)
    block_peak = jnp.max(attention_logits, axis=2)
    weights = jnp.where(live_mask, jnp.exp(attention_logits - block_peak[..., None]), 0.0)
    block_total = jnp.sum(weights, axis=2)
    block_out = jnp.einsum(
        "shp,shpd->shd",
        weights.astype(jnp.bfloat16),
        values_cache,
        preferred_element_type=jnp.float32,
    )
    peak_all, total_all, out_all = merged_2((block_peak, block_total, block_out), "kv", fold_parts)
    own_score = (
        jnp.sum(queries.astype(jnp.float32) * key_new.astype(jnp.float32), axis=2) * score_scale
    )
    top_score = jnp.maximum(peak_all, own_score)
    past_weight = jnp.exp(peak_all - top_score)
    own_weight = jnp.exp(own_score - top_score)
    numerator = (
        out_all * past_weight[..., None] + value_new.astype(jnp.float32) * own_weight[..., None]
    )
    denominator = total_all * past_weight + own_weight
    attended = (numerator / denominator[..., None]).reshape(seqs_here, heads_here * head_dim)
    attended_in = (attended * gain_att.astype(jnp.float32)).astype(jnp.bfloat16)
    part_out = jnp.dot(attended_in, w_out, preferred_element_type=jnp.float32)
    att_squares = jnp.sum(attended * attended, axis=1)
    part_out, att_total = lax.psum((part_out, att_squares), "tp")
    scale_att = lax.rsqrt(att_total / (attended.shape[1] * lax.axis_size("tp")) + norm_eps)[:, None]
    residual = (stream_float + scale_att * part_out).astype(jnp.bfloat16)
    residual_float = residual.astype(jnp.float32)
    mixer_in = (residual_float * gain_mlp.astype(jnp.float32)).astype(jnp.bfloat16)
    mixer_squares = jnp.sum(residual_float * residual_float, axis=1)
    part_up = jnp.dot(mixer_in, w_up, preferred_element_type=jnp.float32)
    pre_act, mixer_total = lax.psum((part_up, mixer_squares), "kv")
    scale_mixer = lax.rsqrt(mixer_total / width_all + norm_eps)[:, None]
    hidden = jnp.square(jax.nn.relu(pre_act * scale_mixer)).astype(jnp.bfloat16)
    part_down = jnp.dot(hidden, w_down, preferred_element_type=jnp.float32)
    mixer_out = lax.psum(part_down, "tp")
    return (residual_float + mixer_out).astype(jnp.bfloat16)


def lanes_of(shape):
    return lax.broadcasted_iota(jnp.int32, shape, 1)


def rows_of(shape):
    return lax.broadcasted_iota(jnp.int32, shape, 0)


def to_column(row, count, *starts):
    shape = (count, LANES)
    apart = lanes_of(shape) - rows_of(shape)
    hit = functools.reduce(jnp.logical_or, [apart == start for start in starts])
    return jnp.sum(
        jnp.where(hit, jnp.broadcast_to(row, shape), 0.0), axis=1, keepdims=True
    )


def to_row(column, start):
    shape = (column.shape[0], LANES)
    hit = lanes_of(shape) - rows_of(shape) == start
    return jnp.sum(
        jnp.where(hit, jnp.broadcast_to(column, shape), 0.0), axis=0, keepdims=True
    )


Q, STAT, KV, Q_ALL, OUT, PEAK, ATT, SQUARE, MIX, GAIN, SWAP_ONE, SWAP_TWO = range(12)
TO_RELAY, STRAIGHT, FROM_RELAY, HID_STRAIGHT, HID_LEVEL, HID_ON = 12, 13, 14, 15, 17, 21
SENDS, ARRIVALS = 22, 29


def layer_kernel(
    kv_n,
    lengths, stream, gain_in, gain_att, gain_mlp, decay,
    w_forget, w_query, w_key, w_value, keys, values, w_out, w_up, w_down,
    out,
    len_s, x_v, gi_v, ga_v, gm_v, decay_v,
    wf_v, wq_v, wk_v, wv_v, keys_v, keys_turned, values_v, wo_v, wu_v, wd_v,
    gain_far, q_send, q_recv, st_send, st_recv, kv_send, kv_recv,
    q_own, q_all, q_float, o_float, o_send, o_recv, pk_send, pk_recv,
    att_own, att_all, sq_own, sq_all, send5, recv5,
    mix_own, mix_all, up_send, relay_recv, relay_send, up_recv,
    hid_relay, hid_all, send8, recv8,
    load_sem, cache_sem, ssem, rsem,
):
    me = lax.axis_index("kv")
    tp = lax.axis_index("tp")
    far = 1 - tp
    seqs, cols = x_v.shape
    heads = decay_v.shape[1]
    pos_here = decay_v.shape[2]
    dim = keys_v.shape[-1]
    rows = q_own.shape[0]
    groups = seqs // rows
    hidden_here = hid_all.shape[2]
    chunks = cache_sem.shape[1]
    per_chunk = seqs // chunks
    width_all = cols * kv_n
    others = kv_n - 1
    score_scale = 1.0 / math.sqrt(dim)
    together = math.gcd(8, per_chunk)

    level, spot = me // PLANE, me % PLANE
    levels = (level, level + 1 - 2 * (level % 2), (level + 2) % 4, 3 - level)
    side, along = spot // 2, spot % 2
    spots = (
        spot, side * 2 + 1 - along, (1 - side) * 2 + along, (1 - side) * 2 + 1 - along
    )
    peers = [levels[k // PLANE] * PLANE + spots[k % PLANE] for k in range(kv_n)]
    far_first = (15, 14, 13, 11, 12, 10, 9, 7, 8, 6, 5, 3, 4, 2, 1, 0)
    plane_order = (3, 1, 2, 0)
    my_group, my_head = me // heads, me % heads

    barrier = pltpu.get_barrier_semaphore()
    for k in far_first:
        pl.semaphore_signal(
            barrier, inc=1, device_id=(peers[k], far), device_id_type=pl.DeviceIdType.MESH
        )

    def load(src, dst, index):
        return pltpu.make_async_copy(src, dst, load_sem.at[index])

    start_row = pl.multiple_of(me * cols, cols)
    first_head = pl.multiple_of(tp * heads, heads)
    first_loads = [
        load(stream, x_v, 0),
        load(gain_in, gi_v, 1),
        load(w_query, wq_v, 2),
        load(w_forget.at[pl.ds(first_head, heads), pl.ds(start_row, cols)], wf_v, 3),
        load(w_key, wk_v, 4),
        load(w_value, wv_v, 5),
    ]
    small_loads = [
        load(gain_att, ga_v, 6), load(decay, decay_v, 7), load(lengths, len_s, 8),
        load(gain_mlp, gm_v, 9),
    ]
    late_loads = [load(w_out, wo_v, 10), load(w_up, wu_v, 11), load(w_down, wd_v, 12)]
    for copy in first_loads:
        copy.start()
    for copy in small_loads:
        copy.start()

    def cache_copy(which, chunk):
        src, dst = ((keys, keys_v), (values, values_v))[which]
        part = pl.ds(chunk * per_chunk, per_chunk)
        return pltpu.make_async_copy(src.at[part], dst.at[part], cache_sem.at[which, chunk])

    def remote(sent, landed, src, dst, device, core):
        return pltpu.make_async_remote_copy(
            src_ref=src, dst_ref=dst, send_sem=ssem.at[sent], recv_sem=rsem.at[landed],
            device_id=(device, core), device_id_type=pl.DeviceIdType.MESH,
        )

    def all_of(index, held):
        return remote(index, index, held, held, me, far)

    def scatter(phase, send, recv, k):
        remote(phase, phase, send.at[peers[k]], recv.at[k], peers[k], far).start()

    def row_to(phase, src, recv, k):
        remote(phase, phase, src, recv.at[pl.ds(k, 1)], peers[k], far).start()

    def spread(phase, own, held, k):
        remote(phase, phase, own, held.at[me], peers[k], far).start()

    for copy in first_loads[:4]:
        copy.wait()
    x = x_v[...].astype(f32)
    scaled = (x * gi_v[...].astype(f32).reshape(1, -1)).astype(bf16)

    def by_owner(dst, part, place):
        for g in range(groups):
            for h in range(heads):
                dst[g * heads + h, place * rows:(place + 1) * rows, :] = part[
                    g * rows:(g + 1) * rows, h * dim:(h + 1) * dim
                ]

    by_owner(q_send, jnp.dot(scaled, wq_v[...], preferred_element_type=f32).astype(bf16), 0)
    squares = x * x
    high = squares.astype(bf16)
    low = (squares - high.astype(f32)).astype(bf16)
    blank = jnp.zeros((32, cols), bf16)
    last = (((1,), (1,)), ((), ()))
    st_send[...] = lax.dot_general(
        jnp.ones((heads, cols), bf16), jnp.concatenate([high, blank, low, blank], axis=0),
        last, preferred_element_type=f32,
    ) + lax.dot_general(
        wf_v[...], jnp.concatenate([blank, scaled, blank, blank], axis=0),
        last, preferred_element_type=f32,
    )
    for copy in first_loads[4:]:
        copy.wait()
    for copy in small_loads:
        copy.wait()
    for chunk in range(chunks):
        cache_copy(0, chunk).start()
    for chunk in range(chunks):
        cache_copy(1, chunk).start()
    for copy in late_loads:
        copy.start()
    pl.semaphore_wait(barrier, kv_n)
    for k in far_first:
        scatter(Q, q_send, q_recv, k)
        row_to(STAT, st_send.at[pl.ds(peers[k] % heads, 1)], st_recv, k)
    gain_swap = remote(GAIN, GAIN, ga_v, gain_far, me, far)
    gain_swap.start()
    for place, weight in enumerate((wk_v, wv_v)):
        by_owner(
            kv_send, jnp.dot(scaled, weight[...], preferred_element_type=f32).astype(bf16), place
        )
    for k in far_first:
        scatter(KV, kv_send, kv_recv, k)
    total = jnp.zeros((rows, dim), f32)

    def turn_chunk(chunk, carry):
        cache_copy(0, chunk).wait()

        def turn(i, c):
            s = chunk * per_chunk + i
            for h in range(heads):
                keys_turned[
                    s, h % 2 * dim:(h % 2 + 1) * dim, h // 2 * pos_here:(h // 2 + 1) * pos_here
                ] = keys_v[s, h].T
            return c

        return lax.fori_loop(0, per_chunk, turn, carry)

    lax.fori_loop(0, chunks // 2, turn_chunk, 0)
    all_of(STAT, st_recv).wait_recv()
    all_of(Q, q_recv).wait_recv()
    for k in range(kv_n):
        total = total + q_recv[k].astype(f32)
    stat_row = jnp.sum(st_recv[...], axis=0, keepdims=True)
    first_lane = my_group * rows
    scale_in = lax.rsqrt(
        to_column(stat_row, rows, first_lane, first_lane + 64) / width_all + norm_eps
    )
    query = (total * scale_in).astype(bf16)
    q_own[...] = query
    for k in far_first:
        spread(Q_ALL, q_own, q_all, k)
    gate = to_column(stat_row, rows, first_lane + 32) * scale_in
    forget = jnp.minimum(gate, 0.0) - jnp.log1p(jnp.exp(-jnp.abs(gate)))

    lax.fori_loop(chunks // 2, chunks, turn_chunk, 0)
    all_of(Q_ALL, q_all).wait_recv()
    q_float[...] = q_all[...].reshape(kv_n * rows, dim).astype(f32)
    head_row = rows_of((heads, pos_here))
    position = me * pos_here + lanes_of((heads, pos_here))
    lane_h = lanes_of((heads, LANES))

    even = rows_of((heads, dim)) % 2 == 0

    def in_pairs(cache, s):
        return jnp.concatenate(
            [
                jnp.concatenate([cache[s, h], cache[s, h + 1]], axis=1)
                for h in range(0, heads, 2)
            ],
            axis=0,
        )

    def some_sequences(first_seq, marks):
        batch = [first_seq + i for i in range(together)]
        places = [
            pl.ds((s // rows) * (heads * rows) + s % rows, heads, stride=rows) for s in batch
        ]
        q_parts = [q_float[mine, :] for mine in places]
        everies = [
            lax.dot_general(
                jnp.concatenate(
                    [jnp.where(even, q_s, 0.0), jnp.where(even, 0.0, q_s)], axis=1
                ).astype(bf16),
                keys_turned[s], (((1,), (0,)), ((), ())), preferred_element_type=f32,
            )
            for q_s, s in zip(q_parts, batch)
        ]
        spreads = []
        for every, s in zip(everies, batch):
            score = every[:, :pos_here]
            for pair in range(1, heads // 2):
                score = jnp.where(
                    head_row // 2 == pair, every[:, pair * pos_here:(pair + 1) * pos_here], score
                )
            score = score * score_scale + decay_v[s]
            live = position < len_s[s]
            score = jnp.where(live, score, masked_score)
            peak = jnp.max(score, axis=1, keepdims=True)
            probs = jnp.where(live, jnp.exp(score - peak), 0.0)
            block_total = jnp.sum(probs, axis=1, keepdims=True)
            spreads.append(jnp.concatenate(
                [jnp.where(head_row // 2 == pair, probs, 0.0) for pair in range(heads // 2)],
                axis=1,
            ).astype(bf16))
            marks = jnp.where(lane_h == s % rows, peak, marks)
            marks = jnp.where(lane_h == s % rows + rows, block_total, marks)
        outs = [
            jnp.dot(part, in_pairs(values_v, s), preferred_element_type=f32)
            for part, s in zip(spreads, batch)
        ]
        for mine, out_s in zip(places, outs):
            o_float[mine, :] = jnp.where(even, out_s[:, :dim], out_s[:, dim:])
        return marks

    def one_chunk(chunk, marks):
        cache_copy(1, chunk).wait()

        def inner(i, c):
            return some_sequences(chunk * per_chunk + together * i, c)

        return lax.fori_loop(0, per_chunk // together, inner, marks)

    group_chunks = chunks // groups
    for g in range(groups):
        marks = lax.fori_loop(
            g * group_chunks, (g + 1) * group_chunks, one_chunk, jnp.zeros((heads, LANES), f32)
        )
        pk_send[g * heads:(g + 1) * heads, :] = marks
    o_send[...] = o_float[...].astype(bf16).reshape(kv_n, rows, dim)
    for k in far_first:
        scatter(OUT, o_send, o_recv, k)
        row_to(PEAK, pk_send.at[pl.ds(peers[k], 1)], pk_recv, k)

    keys_total = jnp.zeros((2 * rows, dim), f32)
    all_of(KV, kv_recv).wait_recv()
    for k in range(kv_n):
        keys_total = keys_total + kv_recv[k].astype(f32)
    key_new = (keys_total[:rows] * scale_in).astype(bf16).astype(f32)
    value_new = (keys_total[rows:] * scale_in).astype(bf16).astype(f32)
    own_score = jnp.sum(query.astype(f32) * key_new, axis=1, keepdims=True) * score_scale
    gain_swap.wait_recv()
    gain_here = gain_far[...].astype(f32).reshape(1, -1)
    gain_head = gain_here[:, :dim]
    for h in range(1, heads):
        gain_head = jnp.where(my_head == h, gain_here[:, h * dim:(h + 1) * dim], gain_head)

    for copy in late_loads:
        copy.wait()
    for index, held in ((Q, q_recv), (STAT, st_recv), (KV, kv_recv), (Q_ALL, q_all)):
        all_of(index, held).wait_send()
    gain_swap.wait_send()
    all_of(PEAK, pk_recv).wait_recv()
    peaks = pk_recv[...]
    top_row = jnp.max(peaks, axis=0, keepdims=True)
    shares = jnp.exp(peaks - top_row)
    total_row = jnp.sum(shares * pltpu.roll(peaks, LANES - rows, 1), axis=0, keepdims=True)
    peak_all = to_column(top_row, rows, 0) + forget
    total_all = to_column(total_row, rows, 0)
    share_columns = [to_column(shares[k:k + 1], rows, 0) for k in range(kv_n)]
    top = jnp.maximum(peak_all, own_score)
    past_weight = jnp.exp(peak_all - top)
    own_weight = jnp.exp(own_score - top)
    out_all = jnp.zeros((rows, dim), f32)
    all_of(OUT, o_recv).wait_recv()
    for k in range(kv_n):
        out_all = out_all + share_columns[k] * o_recv[k].astype(f32)
    attended_one = (out_all * past_weight + value_new * own_weight) / (
        total_all * past_weight + own_weight
    )
    att_own[...] = (attended_one * gain_head).astype(bf16)
    squares_one = jnp.sum(attended_one * attended_one, axis=1, keepdims=True)
    sq_own[...] = jnp.broadcast_to(to_row(squares_one, first_lane), sq_own.shape)
    for k in far_first:
        spread(ATT, att_own, att_all, k)
        row_to(SQUARE, sq_own.at[pl.ds(0, 1)], sq_all, k)

    all_of(ATT, att_all).wait_recv()
    all_of(SQUARE, sq_all).wait_recv()
    attended_in = jnp.concatenate(
        [
            jnp.concatenate([att_all[g * heads + h] for g in range(groups)], axis=0)
            for h in range(heads)
        ],
        axis=1,
    )
    part_out = jnp.dot(attended_in, wo_v[...], preferred_element_type=f32)
    att_squares = to_column(jnp.sum(sq_all[...], axis=0, keepdims=True), seqs, 0)
    send5[:, :cols] = part_out
    send5[:, cols:] = jnp.broadcast_to(att_squares, (seqs, LANES))
    swap5 = remote(SWAP_ONE, SWAP_ONE, send5, recv5, me, far)
    swap5.start()
    swap5.wait_recv()
    width_att = attended_in.shape[1] * 2
    scale_att = lax.rsqrt((att_squares + recv5[:, cols:cols + 1]) / width_att + norm_eps)
    residual = (
        x_v[...].astype(f32) + scale_att * (part_out + recv5[:, :cols])
    ).astype(bf16).astype(f32)
    mixer_in = (residual * gm_v[...].astype(f32).reshape(1, -1)).astype(bf16)
    mixer_squares = jnp.sum(residual * residual, axis=1, keepdims=True)

    def up(apart):
        width = PLANE * hidden_here
        columns = pl.ds(pl.multiple_of(levels[apart] * width, LANES), width)
        return jnp.dot(mixer_in, wu_v[:, columns], preferred_element_type=f32)

    def store_up(apart):
        part = up(apart).astype(bf16)
        for place in range(PLANE):
            up_send[apart * PLANE + place] = part[
                :, place * hidden_here:(place + 1) * hidden_here
            ]

    def to_relay(p):
        return remote(
            TO_RELAY, TO_RELAY, up_send.at[2 * PLANE + spots[p]], relay_recv.at[p], peers[p], far
        )

    from_relay = remote(
        FROM_RELAY, FROM_RELAY, relay_send, up_recv.at[others - PLANE], peers[2 * PLANE], far
    )

    def straight(k):
        apart, p = k // PLANE, k % PLANE
        slot = k - 1 if k < 2 * PLANE else k - 1 - PLANE
        return remote(
            STRAIGHT, STRAIGHT, up_send.at[apart * PLANE + spots[p]], up_recv.at[slot],
            peers[k], tp,
        )

    store_up(2)
    for p in plane_order:
        to_relay(p).start()
    store_up(3)
    for p in plane_order:
        straight(3 * PLANE + p).start()
    mix_own[...] = jnp.broadcast_to(to_row(mixer_squares, 0), mix_own.shape)
    for k in far_first:
        row_to(MIX, mix_own.at[pl.ds(0, 1)], mix_all, k)
    store_up(1)
    for p in plane_order:
        straight(PLANE + p).start()
    store_up(0)
    for p in plane_order[:-1]:
        straight(p).start()
    pre_act = up_send[spot].astype(f32)
    all_of(TO_RELAY, relay_recv).wait_recv()
    relayed = relay_recv[0].astype(f32)
    for p in range(1, PLANE):
        relayed = relayed + relay_recv[p].astype(f32)
    relay_send[...] = relayed.astype(bf16)
    from_relay.start()
    for index, held in ((OUT, o_recv), (PEAK, pk_recv), (ATT, att_all), (SQUARE, sq_all)):
        all_of(index, held).wait_send()
    swap5.wait_send()
    all_of(MIX, mix_all).wait_recv()
    mixer_total = to_column(jnp.sum(mix_all[...], axis=0, keepdims=True), seqs, 0)
    scale_mixer = lax.rsqrt(mixer_total / width_all + norm_eps)
    all_of(STRAIGHT, up_recv.at[pl.ds(0, others - PLANE)]).wait_recv()
    for slot in range(others - PLANE):
        pre_act = pre_act + up_recv[slot].astype(f32)
    from_relay.wait_recv()
    pre_act = pre_act + up_recv[others - PLANE].astype(f32)
    hidden = jnp.maximum(pre_act * scale_mixer, 0.0)
    hid_all[me] = (hidden * hidden).astype(bf16)

    half = seqs // 2

    def to_level(apart, part):
        some = pl.ds(part * half, half)
        return remote(
            HID_LEVEL, HID_LEVEL + 2 * (apart - 2) + part, hid_all.at[me, some],
            hid_relay.at[apart - 2, some], peers[apart * PLANE], far,
        )

    def onward(apart, part, p):
        some = pl.ds(part * half, half)
        return remote(
            HID_ON, HID_ON + (apart - 2) * PLANE + p, hid_relay.at[apart - 2, some],
            hid_all.at[peers[apart * PLANE], some], peers[p], far,
        )

    def arrived(k):
        index = HID_ON + k - 2 * PLANE
        return remote(index, index, hid_all.at[me], hid_all.at[peers[k]], peers[k], tp)

    for part in (0, 1):
        for apart in (2, 3):
            to_level(apart, part).start()
    for apart in (0, 1):
        for p in plane_order:
            k = apart * PLANE + p
            if k:
                remote(
                    HID_STRAIGHT, HID_STRAIGHT + apart, hid_all.at[me], hid_all.at[me],
                    peers[k], tp,
                ).start()

    def down(owner):
        depth = pl.ds(pl.multiple_of(owner * hidden_here, LANES), hidden_here)
        return jnp.dot(hid_all[owner], wd_v[depth, :], preferred_element_type=f32)

    part_down = down(me)
    for part in (0, 1):
        for apart in (2, 3):
            to_level(apart, part).wait_recv()
            for p in plane_order:
                onward(apart, part, p).start()
    blocks = up_send.at[pl.ds(0, PLANE - 1)], up_send.at[pl.ds(0, PLANE)]
    for apart in (0, 1):
        all_of(HID_STRAIGHT + apart, blocks[apart]).wait_recv()
        for p in range(PLANE):
            if apart + p:
                part_down = part_down + down(peers[apart * PLANE + p])
    all_of(MIX, mix_all).wait_send()
    all_of(TO_RELAY, relay_recv).wait_send()
    all_of(STRAIGHT, up_recv.at[pl.ds(0, others - PLANE)]).wait_send()
    from_relay.wait_send()
    all_of(HID_LEVEL, hid_relay).wait_send()
    all_of(HID_STRAIGHT, up_send.at[pl.ds(0, 2 * PLANE - 1)]).wait_send()
    for k in (8, 9, 10, 11, 12, 13, 14, 15):
        arrived(k).wait_recv()
        part_down = part_down + down(peers[k])
    send8[...] = part_down
    swap8 = remote(SWAP_TWO, SWAP_TWO, send8, recv8, me, far)
    swap8.start()
    all_of(HID_ON, up_send.at[pl.ds(0, 2 * PLANE)]).wait_send()
    swap8.wait_recv()
    out[...] = (residual + (part_down + recv8[...])).astype(bf16)
    swap8.wait_send()


def fits(kv_n, tp_n, seqs, cols, heads, heads_all, pos_here, dim, units):
    if tp_n != 2 or kv_n != PLANE * PLANE or heads != 8 or seqs != 32:
        return False
    return (
        cols % LANES == 0 and pos_here == LANES and dim == LANES
        and heads_all == 2 * heads and units % (kv_n * LANES) == 0
    )


def layer(
    stream, gain_in, w_query, w_key, w_value, w_forget, keys_cache, values_cache,
    decay_cache, lengths, gain_att, w_out, gain_mlp, w_up, w_down,
):
    kv_n, tp_n = lax.axis_size("kv"), lax.axis_size("tp")
    seqs, cols = stream.shape
    heads, pos_here, dim = keys_cache.shape[1:]
    heads_all = w_forget.shape[1]
    units = w_up.shape[1]
    if not fits(kv_n, tp_n, seqs, cols, heads, heads_all, pos_here, dim, units):
        return per_device(
            stream, gain_in, w_query, w_key, w_value, w_forget, keys_cache, values_cache,
            decay_cache, lengths, gain_att, w_out, gain_mlp, w_up, w_down,
        )
    rows = seqs * heads // kv_n
    hidden_here = units // kv_n
    chunks = 4
    anywhere = pl.BlockSpec(memory_space=pl.ANY)

    def held(*shape, kind=bf16):
        return pltpu.VMEM(shape, kind)

    return pl.pallas_call(
        functools.partial(layer_kernel, kv_n),
        out_shape=pltpu.VMEM((seqs, cols), bf16),
        in_specs=[anywhere] * 15,
        out_specs=pl.BlockSpec(memory_space=pltpu.VMEM),
        scratch_shapes=[
            pltpu.SMEM((seqs,), jnp.int32),
            held(seqs, cols),
            held(cols),
            held(*gain_att.shape),
            held(cols),
            held(*decay_cache.shape, kind=f32),
            held(heads, cols),
            held(*w_query.shape),
            held(*w_key.shape),
            held(*w_value.shape),
            held(*keys_cache.shape),
            held(seqs, 2 * dim, heads // 2 * pos_here),
            held(*values_cache.shape),
            held(*w_out.shape),
            held(*w_up.shape),
            held(*w_down.shape),
            held(*gain_att.shape),
            held(kv_n, rows, dim),
            held(kv_n, rows, dim),
            held(heads, LANES, kind=f32),
            held(kv_n, LANES, kind=f32),
            held(kv_n, 2 * rows, dim),
            held(kv_n, 2 * rows, dim),
            held(rows, dim),
            held(kv_n, rows, dim),
            held(kv_n * rows, dim, kind=f32),
            held(kv_n * rows, dim, kind=f32),
            held(kv_n, rows, dim),
            held(kv_n, rows, dim),
            held(kv_n, LANES, kind=f32),
            held(kv_n, LANES, kind=f32),
            held(rows, dim),
            held(kv_n, rows, dim),
            held(8, LANES, kind=f32),
            held(kv_n, LANES, kind=f32),
            held(seqs, cols + LANES, kind=f32),
            held(seqs, cols + LANES, kind=f32),
            held(8, LANES, kind=f32),
            held(kv_n, LANES, kind=f32),
            held(kv_n, seqs, hidden_here),
            held(PLANE, seqs, hidden_here),
            held(seqs, hidden_here),
            held(kv_n - PLANE, seqs, hidden_here),
            held(2, seqs, hidden_here),
            held(kv_n, seqs, hidden_here),
            held(seqs, cols, kind=f32),
            held(seqs, cols, kind=f32),
            pltpu.SemaphoreType.DMA((13,)),
            pltpu.SemaphoreType.DMA((2, chunks)),
            pltpu.SemaphoreType.DMA((SENDS,)),
            pltpu.SemaphoreType.DMA((ARRIVALS,)),
        ],
        compiler_params=pltpu.CompilerParams(
            collective_id=0, has_side_effects=True, vmem_limit_bytes=60 * 1024 * 1024
        ),
    )(
        lengths, stream, gain_in, gain_att,
        gain_mlp, decay_cache,
        w_forget.T, w_query, w_key, w_value, keys_cache, values_cache, w_out, w_up, w_down,
    )


def solution(mesh):
    in_specs = (
        P(None, "kv"),
        P("kv"),
        P("kv", "tp"),
        P("kv", "tp"),
        P("kv", "tp"),
        P(),
        P(None, "tp", "kv", None),
        P(None, "tp", "kv", None),
        P(None, "tp", "kv"),
        P(),
        P("tp"),
        P("tp", "kv"),
        P("kv"),
        P("kv", "tp"),
        P("tp", "kv"),
    )
    out_specs = P(None, "kv")
    return jax.shard_map(
        layer, mesh=mesh, in_specs=in_specs, out_specs=out_specs, check_vma=False
    )
```

```python
import functools
import math

import jax
import jax.numpy as jnp
from jax import lax
from jax.experimental import pallas as pl
from jax.experimental.pallas import tpu as pltpu
from jax.sharding import PartitionSpec as P

f32 = jnp.float32
bf16 = jnp.bfloat16
LANES = 128
PLANE = 4

norm_eps = 1e-06
masked_score = -1e30


def merged_2(value, axis, join):
    pieces = jax.tree.map(lambda part: lax.all_gather(part, axis), value)
    head = jax.tree.map(lambda part: part[0], pieces)
    tail = jax.tree.map(lambda part: part[1:], pieces)
    so_far, _ = lax.scan(lambda so_far, share: (join(so_far, share), None), head, tail)
    return so_far


def fold_parts(left_part, right_part):
    peak_all = jnp.maximum(left_part[0], right_part[0])
    weight_one = jnp.exp(left_part[0] - peak_all)
    weight_two = jnp.exp(right_part[0] - peak_all)
    total_sum = left_part[1] * weight_one + right_part[1] * weight_two
    merged = left_part[2] * weight_one[..., None] + right_part[2] * weight_two[..., None]
    return (peak_all, total_sum, merged)


def per_device(
    stream,
    gain_in,
    w_query,
    w_key,
    w_value,
    w_forget,
    keys_cache,
    values_cache,
    decay_cache,
    lengths,
    gain_att,
    w_out,
    gain_mlp,
    w_up,
    w_down,
):
    kv_index = lax.axis_index("kv")
    tp_index = lax.axis_index("tp")
    kv_count = lax.axis_size("kv")
    seqs_here, cols_here = stream.shape
    heads_here = keys_cache.shape[1]
    pos_here = keys_cache.shape[2]
    head_dim = keys_cache.shape[3]
    width_all = cols_here * kv_count
    score_scale = 1.0 / math.sqrt(head_dim)
    stream_float = stream.astype(jnp.float32)
    scaled = (stream_float * gain_in.astype(jnp.float32)).astype(jnp.bfloat16)
    square_sum = jnp.sum(stream_float * stream_float, axis=1)
    forget_rows = lax.dynamic_slice(
        w_forget, (kv_index * cols_here, tp_index * heads_here), (cols_here, heads_here)
    )
    part_query = jnp.dot(scaled, w_query, preferred_element_type=jnp.float32)
    part_key = jnp.dot(scaled, w_key, preferred_element_type=jnp.float32)
    part_value = jnp.dot(scaled, w_value, preferred_element_type=jnp.float32)
    part_forget = jnp.dot(scaled, forget_rows, preferred_element_type=jnp.float32)
    part_query, part_key, part_value, part_forget, square_total = lax.psum(
        (part_query, part_key, part_value, part_forget, square_sum), "kv"
    )
    scale_in = lax.rsqrt(square_total / width_all + norm_eps)[:, None]
    queries = (part_query * scale_in).astype(jnp.bfloat16).reshape(seqs_here, heads_here, head_dim)
    key_new = (part_key * scale_in).astype(jnp.bfloat16).reshape(seqs_here, heads_here, head_dim)
    value_new = (
        (part_value * scale_in).astype(jnp.bfloat16).reshape(seqs_here, heads_here, head_dim)
    )
    forget = jax.nn.log_sigmoid(part_forget * scale_in)
    attention_logits = (
        jnp.einsum("shd,shpd->shp", queries, keys_cache, preferred_element_type=jnp.float32)
        * score_scale
    )
    attention_logits = attention_logits + forget[:, :, None] + decay_cache
    cache_positions = kv_index * pos_here + lax.iota(jnp.int32, pos_here)
    live_mask = (cache_positions[None, :] < lengths[:, None])[:, None, :]
    attention_logits = jnp.where(live_mask, attention_logits, masked_score)
    block_peak = jnp.max(attention_logits, axis=2)
    weights = jnp.where(live_mask, jnp.exp(attention_logits - block_peak[..., None]), 0.0)
    block_total = jnp.sum(weights, axis=2)
    block_out = jnp.einsum(
        "shp,shpd->shd",
        weights.astype(jnp.bfloat16),
        values_cache,
        preferred_element_type=jnp.float32,
    )
    peak_all, total_all, out_all = merged_2((block_peak, block_total, block_out), "kv", fold_parts)
    own_score = (
        jnp.sum(queries.astype(jnp.float32) * key_new.astype(jnp.float32), axis=2) * score_scale
    )
    top_score = jnp.maximum(peak_all, own_score)
    past_weight = jnp.exp(peak_all - top_score)
    own_weight = jnp.exp(own_score - top_score)
    numerator = (
        out_all * past_weight[..., None] + value_new.astype(jnp.float32) * own_weight[..., None]
    )
    denominator = total_all * past_weight + own_weight
    attended = (numerator / denominator[..., None]).reshape(seqs_here, heads_here * head_dim)
    attended_in = (attended * gain_att.astype(jnp.float32)).astype(jnp.bfloat16)
    part_out = jnp.dot(attended_in, w_out, preferred_element_type=jnp.float32)
    att_squares = jnp.sum(attended * attended, axis=1)
    part_out, att_total = lax.psum((part_out, att_squares), "tp")
    scale_att = lax.rsqrt(att_total / (attended.shape[1] * lax.axis_size("tp")) + norm_eps)[:, None]
    residual = (stream_float + scale_att * part_out).astype(jnp.bfloat16)
    residual_float = residual.astype(jnp.float32)
    mixer_in = (residual_float * gain_mlp.astype(jnp.float32)).astype(jnp.bfloat16)
    mixer_squares = jnp.sum(residual_float * residual_float, axis=1)
    part_up = jnp.dot(mixer_in, w_up, preferred_element_type=jnp.float32)
    pre_act, mixer_total = lax.psum((part_up, mixer_squares), "kv")
    scale_mixer = lax.rsqrt(mixer_total / width_all + norm_eps)[:, None]
    hidden = jnp.square(jax.nn.relu(pre_act * scale_mixer)).astype(jnp.bfloat16)
    part_down = jnp.dot(hidden, w_down, preferred_element_type=jnp.float32)
    mixer_out = lax.psum(part_down, "tp")
    return (residual_float + mixer_out).astype(jnp.bfloat16)


def lanes_of(shape):
    return lax.broadcasted_iota(jnp.int32, shape, 1)


def rows_of(shape):
    return lax.broadcasted_iota(jnp.int32, shape, 0)


def to_column(row, count, *starts):
    shape = (count, LANES)
    apart = lanes_of(shape) - rows_of(shape)
    hit = functools.reduce(jnp.logical_or, [apart == start for start in starts])
    return jnp.sum(
        jnp.where(hit, jnp.broadcast_to(row, shape), 0.0), axis=1, keepdims=True
    )


def to_row(column, start):
    shape = (column.shape[0], LANES)
    hit = lanes_of(shape) - rows_of(shape) == start
    return jnp.sum(
        jnp.where(hit, jnp.broadcast_to(column, shape), 0.0), axis=0, keepdims=True
    )


Q, STAT, KV, Q_ALL, OUT, PEAK, ATT, SQUARE, MIX, GAIN, SWAP_ONE, SWAP_TWO = range(12)
TO_RELAY, STRAIGHT, FROM_RELAY, HID_STRAIGHT, HID_LEVEL, HID_ON = 12, 13, 14, 15, 17, 21
SENDS, ARRIVALS, STRAIGHT_OWN = 22, 30, 29


def layer_kernel(
    kv_n,
    lengths, stream, gain_in, gain_att, gain_mlp, decay,
    w_forget, w_query, w_key, w_value, keys, values, w_out, w_up, w_down,
    out,
    len_s, x_v, gi_v, ga_v, gm_v, decay_v,
    wf_v, wq_v, wk_v, wv_v, keys_v, keys_turned, values_v, wo_v, wu_v, wd_v,
    gain_far, q_send, q_recv, st_send, st_recv, kv_send, kv_recv,
    q_own, q_all, q_float, o_float, o_send, o_recv, pk_send, pk_recv,
    att_own, att_all, sq_own, sq_all, send5, recv5,
    mix_own, mix_all, up_send, relay_recv, relay_send, up_recv,
    hid_all, send8, recv8,
    load_sem, cache_sem, ssem, rsem,
):
    me = lax.axis_index("kv")
    tp = lax.axis_index("tp")
    far = 1 - tp
    seqs, cols = x_v.shape
    heads = decay_v.shape[1]
    pos_here = decay_v.shape[2]
    dim = keys_v.shape[-1]
    rows = q_own.shape[0]
    groups = seqs // rows
    hidden_here = hid_all.shape[2]
    chunks = cache_sem.shape[1]
    per_chunk = seqs // chunks
    width_all = cols * kv_n
    others = kv_n - 1
    score_scale = 1.0 / math.sqrt(dim)
    together = math.gcd(8, per_chunk)

    level, spot = me // PLANE, me % PLANE
    levels = (level, level + 1 - 2 * (level % 2), (level + 2) % 4, 3 - level)
    side, along = spot // 2, spot % 2
    spots = (
        spot, side * 2 + 1 - along, (1 - side) * 2 + along, (1 - side) * 2 + 1 - along
    )
    peers = [levels[k // PLANE] * PLANE + spots[k % PLANE] for k in range(kv_n)]
    far_first = (15, 14, 13, 11, 12, 10, 9, 7, 8, 6, 5, 3, 4, 2, 1, 0)
    plane_order = (3, 1, 2, 0)
    my_group, my_head = me // heads, me % heads

    barrier = pltpu.get_barrier_semaphore()
    for k in far_first:
        pl.semaphore_signal(
            barrier, inc=1, device_id=(peers[k], far), device_id_type=pl.DeviceIdType.MESH
        )

    def load(src, dst, index):
        return pltpu.make_async_copy(src, dst, load_sem.at[index])

    start_row = pl.multiple_of(me * cols, cols)
    first_head = pl.multiple_of(tp * heads, heads)
    first_loads = [
        load(stream, x_v, 0),
        load(gain_in, gi_v, 1),
        load(w_query, wq_v, 2),
        load(w_forget.at[pl.ds(first_head, heads), pl.ds(start_row, cols)], wf_v, 3),
        load(w_key, wk_v, 4),
        load(w_value, wv_v, 5),
    ]
    small_loads = [
        load(gain_att, ga_v, 6), load(decay, decay_v, 7), load(lengths, len_s, 8),
        load(gain_mlp, gm_v, 9),
    ]
    late_loads = [load(w_out, wo_v, 10), load(w_up, wu_v, 11), load(w_down, wd_v, 12)]
    for copy in first_loads:
        copy.start()
    for copy in small_loads:
        copy.start()

    def cache_copy(which, chunk):
        src, dst = ((keys, keys_v), (values, values_v))[which]
        part = pl.ds(chunk * per_chunk, per_chunk)
        return pltpu.make_async_copy(src.at[part], dst.at[part], cache_sem.at[which, chunk])

    def remote(sent, landed, src, dst, device, core):
        return pltpu.make_async_remote_copy(
            src_ref=src, dst_ref=dst, send_sem=ssem.at[sent], recv_sem=rsem.at[landed],
            device_id=(device, core), device_id_type=pl.DeviceIdType.MESH,
        )

    def all_of(index, held):
        return remote(index, index, held, held, me, far)

    def scatter(phase, send, recv, k):
        remote(phase, phase, send.at[peers[k]], recv.at[k], peers[k], far).start()

    def row_to(phase, src, recv, k):
        remote(phase, phase, src, recv.at[pl.ds(k, 1)], peers[k], far).start()

    def spread(phase, own, held, k):
        remote(phase, phase, own, held.at[me], peers[k], far).start()

    for copy in first_loads[:4]:
        copy.wait()
    x = x_v[...].astype(f32)
    scaled = (x * gi_v[...].astype(f32).reshape(1, -1)).astype(bf16)

    def by_owner(dst, part, place):
        for g in range(groups):
            for h in range(heads):
                dst[g * heads + h, place * rows:(place + 1) * rows, :] = part[
                    g * rows:(g + 1) * rows, h * dim:(h + 1) * dim
                ]

    by_owner(q_send, jnp.dot(scaled, wq_v[...], preferred_element_type=f32).astype(bf16), 0)
    squares = x * x
    high = squares.astype(bf16)
    low = (squares - high.astype(f32)).astype(bf16)
    blank = jnp.zeros((32, cols), bf16)
    last = (((1,), (1,)), ((), ()))
    st_send[...] = lax.dot_general(
        jnp.ones((heads, cols), bf16), jnp.concatenate([high, blank, low, blank], axis=0),
        last, preferred_element_type=f32,
    ) + lax.dot_general(
        wf_v[...], jnp.concatenate([blank, scaled, blank, blank], axis=0),
        last, preferred_element_type=f32,
    )
    for copy in first_loads[4:]:
        copy.wait()
    for copy in small_loads:
        copy.wait()
    for chunk in range(chunks):
        cache_copy(0, chunk).start()
    for chunk in range(chunks):
        cache_copy(1, chunk).start()
    for copy in late_loads:
        copy.start()
    pl.semaphore_wait(barrier, kv_n)
    for k in far_first:
        scatter(Q, q_send, q_recv, k)
        row_to(STAT, st_send.at[pl.ds(peers[k] % heads, 1)], st_recv, k)
    gain_swap = remote(GAIN, GAIN, ga_v, gain_far, me, far)
    gain_swap.start()
    for place, weight in enumerate((wk_v, wv_v)):
        by_owner(
            kv_send, jnp.dot(scaled, weight[...], preferred_element_type=f32).astype(bf16), place
        )
    total = jnp.zeros((rows, dim), f32)

    def turn_chunk(chunk, carry):
        cache_copy(0, chunk).wait()

        def turn(i, c):
            s = chunk * per_chunk + i
            for h in range(heads):
                keys_turned[
                    s, h % 2 * dim:(h % 2 + 1) * dim, h // 2 * pos_here:(h // 2 + 1) * pos_here
                ] = keys_v[s, h].T
            return c

        return lax.fori_loop(0, per_chunk, turn, carry)

    lax.fori_loop(0, chunks // 2, turn_chunk, 0)
    all_of(STAT, st_recv).wait_recv()
    all_of(Q, q_recv).wait_recv()
    for k in range(kv_n):
        total = total + q_recv[k].astype(f32)
    stat_row = jnp.sum(st_recv[...], axis=0, keepdims=True)
    first_lane = my_group * rows
    scale_in = lax.rsqrt(
        to_column(stat_row, rows, first_lane, first_lane + 64) / width_all + norm_eps
    )
    query = (total * scale_in).astype(bf16)
    q_own[...] = query
    for k in far_first:
        spread(Q_ALL, q_own, q_all, k)
    for k in far_first:
        scatter(KV, kv_send, kv_recv, k)
    gate = to_column(stat_row, rows, first_lane + 32) * scale_in
    forget = jnp.minimum(gate, 0.0) - jnp.log1p(jnp.exp(-jnp.abs(gate)))

    lax.fori_loop(chunks // 2, chunks, turn_chunk, 0)
    all_of(Q_ALL, q_all).wait_recv()
    q_float[...] = q_all[...].reshape(kv_n * rows, dim).astype(f32)
    head_row = rows_of((heads, pos_here))
    position = me * pos_here + lanes_of((heads, pos_here))
    lane_h = lanes_of((heads, LANES))

    even = rows_of((heads, dim)) % 2 == 0

    def in_pairs(cache, s):
        return jnp.concatenate(
            [
                jnp.concatenate([cache[s, h], cache[s, h + 1]], axis=1)
                for h in range(0, heads, 2)
            ],
            axis=0,
        )

    def some_sequences(first_seq, marks):
        batch = [first_seq + i for i in range(together)]
        places = [
            pl.ds((s // rows) * (heads * rows) + s % rows, heads, stride=rows) for s in batch
        ]
        q_parts = [q_float[mine, :] for mine in places]
        everies = [
            lax.dot_general(
                jnp.concatenate(
                    [jnp.where(even, q_s, 0.0), jnp.where(even, 0.0, q_s)], axis=1
                ).astype(bf16),
                keys_turned[s], (((1,), (0,)), ((), ())), preferred_element_type=f32,
            )
            for q_s, s in zip(q_parts, batch)
        ]
        spreads = []
        for every, s in zip(everies, batch):
            score = every[:, :pos_here]
            for pair in range(1, heads // 2):
                score = jnp.where(
                    head_row // 2 == pair, every[:, pair * pos_here:(pair + 1) * pos_here], score
                )
            score = score * score_scale + decay_v[s]
            live = position < len_s[s]
            score = jnp.where(live, score, masked_score)
            peak = jnp.max(score, axis=1, keepdims=True)
            probs = jnp.where(live, jnp.exp(score - peak), 0.0)
            block_total = jnp.sum(probs, axis=1, keepdims=True)
            spreads.append(jnp.concatenate(
                [jnp.where(head_row // 2 == pair, probs, 0.0) for pair in range(heads // 2)],
                axis=1,
            ).astype(bf16))
            marks = jnp.where(lane_h == s % rows, peak, marks)
            marks = jnp.where(lane_h == s % rows + rows, block_total, marks)
        outs = [
            jnp.dot(part, in_pairs(values_v, s), preferred_element_type=f32)
            for part, s in zip(spreads, batch)
        ]
        for mine, out_s in zip(places, outs):
            o_float[mine, :] = jnp.where(even, out_s[:, :dim], out_s[:, dim:])
        return marks

    def one_chunk(chunk, marks):
        cache_copy(1, chunk).wait()

        def inner(i, c):
            return some_sequences(chunk * per_chunk + together * i, c)

        return lax.fori_loop(0, per_chunk // together, inner, marks)

    group_chunks = chunks // groups
    for g in range(groups):
        marks = lax.fori_loop(
            g * group_chunks, (g + 1) * group_chunks, one_chunk, jnp.zeros((heads, LANES), f32)
        )
        mine = slice(g * heads, (g + 1) * heads)
        pk_send[mine, :] = marks
        o_send[mine] = o_float[g * heads * rows:(g + 1) * heads * rows, :].astype(bf16).reshape(
            heads, rows, dim
        )
        for step in (1, 0):
            for p in plane_order:
                owner = (g * 2 + (level + step) % 2) * PLANE + spots[p]
                remote(OUT, OUT, o_send.at[owner], o_recv.at[me], owner, far).start()
                remote(
                    PEAK, PEAK, pk_send.at[pl.ds(owner, 1)], pk_recv.at[pl.ds(me, 1)], owner, far
                ).start()

    keys_total = jnp.zeros((2 * rows, dim), f32)
    all_of(KV, kv_recv).wait_recv()
    for k in range(kv_n):
        keys_total = keys_total + kv_recv[k].astype(f32)
    key_new = (keys_total[:rows] * scale_in).astype(bf16).astype(f32)
    value_new = (keys_total[rows:] * scale_in).astype(bf16).astype(f32)
    own_score = jnp.sum(query.astype(f32) * key_new, axis=1, keepdims=True) * score_scale
    gain_swap.wait_recv()
    gain_here = gain_far[...].astype(f32).reshape(1, -1)
    gain_head = gain_here[:, :dim]
    for h in range(1, heads):
        gain_head = jnp.where(my_head == h, gain_here[:, h * dim:(h + 1) * dim], gain_head)

    for copy in late_loads:
        copy.wait()
    for index, held in ((Q, q_recv), (STAT, st_recv), (KV, kv_recv), (Q_ALL, q_all)):
        all_of(index, held).wait_send()
    gain_swap.wait_send()
    all_of(PEAK, pk_recv).wait_recv()
    peaks = pk_recv[...]
    top_row = jnp.max(peaks, axis=0, keepdims=True)
    shares = jnp.exp(peaks - top_row)
    total_row = jnp.sum(shares * pltpu.roll(peaks, LANES - rows, 1), axis=0, keepdims=True)
    peak_all = to_column(top_row, rows, 0) + forget
    total_all = to_column(total_row, rows, 0)
    share_columns = [to_column(shares[k:k + 1], rows, 0) for k in range(kv_n)]
    top = jnp.maximum(peak_all, own_score)
    past_weight = jnp.exp(peak_all - top)
    own_weight = jnp.exp(own_score - top)
    out_all = jnp.zeros((rows, dim), f32)
    all_of(OUT, o_recv).wait_recv()
    for k in range(kv_n):
        out_all = out_all + share_columns[k] * o_recv[k].astype(f32)
    attended_one = (out_all * past_weight + value_new * own_weight) / (
        total_all * past_weight + own_weight
    )
    att_own[...] = (attended_one * gain_head).astype(bf16)
    squares_one = jnp.sum(attended_one * attended_one, axis=1, keepdims=True)
    sq_own[...] = jnp.broadcast_to(to_row(squares_one, first_lane), sq_own.shape)
    for k in far_first:
        spread(ATT, att_own, att_all, k)
        row_to(SQUARE, sq_own.at[pl.ds(0, 1)], sq_all, k)

    all_of(ATT, att_all).wait_recv()
    all_of(SQUARE, sq_all).wait_recv()
    attended_in = jnp.concatenate(
        [
            jnp.concatenate([att_all[g * heads + h] for g in range(groups)], axis=0)
            for h in range(heads)
        ],
        axis=1,
    )
    part_out = jnp.dot(attended_in, wo_v[...], preferred_element_type=f32)
    att_squares = to_column(jnp.sum(sq_all[...], axis=0, keepdims=True), seqs, 0)
    send5[:, :cols] = part_out
    send5[:, cols:] = jnp.broadcast_to(att_squares, (seqs, LANES))
    swap5 = remote(SWAP_ONE, SWAP_ONE, send5, recv5, me, far)
    swap5.start()
    swap5.wait_recv()
    width_att = attended_in.shape[1] * 2
    scale_att = lax.rsqrt((att_squares + recv5[:, cols:cols + 1]) / width_att + norm_eps)
    residual = (
        x_v[...].astype(f32) + scale_att * (part_out + recv5[:, :cols])
    ).astype(bf16).astype(f32)
    mixer_in = (residual * gm_v[...].astype(f32).reshape(1, -1)).astype(bf16)
    mixer_squares = jnp.sum(residual * residual, axis=1, keepdims=True)

    def up(apart):
        width = PLANE * hidden_here
        columns = pl.ds(pl.multiple_of(levels[apart] * width, LANES), width)
        return jnp.dot(mixer_in, wu_v[:, columns], preferred_element_type=f32)

    def store_up(apart):
        part = up(apart).astype(bf16)
        for place in range(PLANE):
            up_send[apart * PLANE + place] = part[
                :, place * hidden_here:(place + 1) * hidden_here
            ]

    def to_relay(p):
        return remote(
            TO_RELAY, TO_RELAY, up_send.at[2 * PLANE + spots[p]], relay_recv.at[p], peers[p], far
        )

    from_relay = remote(
        FROM_RELAY, FROM_RELAY, relay_send, up_recv.at[others - PLANE], peers[2 * PLANE], far
    )

    def straight(k):
        apart, p = k // PLANE, k % PLANE
        slot = k - 1 if k < 2 * PLANE else k - 1 - PLANE
        return remote(
            STRAIGHT, STRAIGHT_OWN if k < PLANE else STRAIGHT,
            up_send.at[apart * PLANE + spots[p]], up_recv.at[slot],
            peers[k], tp,
        )

    store_up(2)
    for p in plane_order:
        to_relay(p).start()
    store_up(3)
    for p in plane_order:
        straight(3 * PLANE + p).start()
    mix_own[...] = jnp.broadcast_to(to_row(mixer_squares, 0), mix_own.shape)
    for k in far_first:
        row_to(MIX, mix_own.at[pl.ds(0, 1)], mix_all, k)
    store_up(1)
    for p in plane_order:
        straight(PLANE + p).start()
    store_up(0)
    for p in plane_order[:-1]:
        straight(p).start()
    pre_act = up_send[spot].astype(f32)
    all_of(TO_RELAY, relay_recv).wait_recv()
    relayed = relay_recv[0].astype(f32)
    for p in range(1, PLANE):
        relayed = relayed + relay_recv[p].astype(f32)
    relay_send[...] = relayed.astype(bf16)
    from_relay.start()
    for index, held in ((OUT, o_recv), (PEAK, pk_recv), (ATT, att_all), (SQUARE, sq_all)):
        all_of(index, held).wait_send()
    swap5.wait_send()
    all_of(MIX, mix_all).wait_recv()
    mixer_total = to_column(jnp.sum(mix_all[...], axis=0, keepdims=True), seqs, 0)
    scale_mixer = lax.rsqrt(mixer_total / width_all + norm_eps)
    remote(
        STRAIGHT, STRAIGHT, up_send.at[pl.ds(0, 2 * PLANE)], up_send.at[pl.ds(0, 2 * PLANE)], me, far
    ).wait_recv()
    for slot in range(PLANE - 1, others - PLANE):
        pre_act = pre_act + up_recv[slot].astype(f32)
    from_relay.wait_recv()
    pre_act = pre_act + up_recv[others - PLANE].astype(f32)
    all_of(STRAIGHT_OWN, up_send.at[pl.ds(0, PLANE - 1)]).wait_recv()
    for slot in range(PLANE - 1):
        pre_act = pre_act + up_recv[slot].astype(f32)
    hidden = jnp.maximum(pre_act * scale_mixer, 0.0)
    hid_all[me] = (hidden * hidden).astype(bf16)

    half = seqs // 2

    def to_level(apart, part):
        some = pl.ds(part * half, half)
        return remote(
            HID_LEVEL, HID_LEVEL + 2 * (apart - 2) + part, hid_all.at[me, some],
            hid_all.at[me, some], peers[apart * PLANE], tp,
        )

    def onward(apart, part, p):
        some = pl.ds(part * half, half)
        return remote(
            HID_ON, HID_ON + (apart - 2) * PLANE + p, hid_all.at[peers[apart * PLANE], some],
            hid_all.at[peers[apart * PLANE], some], peers[p], tp,
        )

    def arrived(k):
        index = HID_ON + k - 2 * PLANE
        return remote(index, index, hid_all.at[me], hid_all.at[peers[k]], peers[k], tp)

    for part in (0, 1):
        for apart in (2, 3):
            to_level(apart, part).start()
    for apart in (0, 1):
        for p in plane_order:
            k = apart * PLANE + p
            if k:
                remote(
                    HID_STRAIGHT, HID_STRAIGHT + apart, hid_all.at[me], hid_all.at[me],
                    peers[k], tp,
                ).start()

    def down(owner):
        depth = pl.ds(pl.multiple_of(owner * hidden_here, LANES), hidden_here)
        return jnp.dot(hid_all[owner], wd_v[depth, :], preferred_element_type=f32)

    part_down = down(me)
    for part in (0, 1):
        for apart in (2, 3):
            to_level(apart, part).wait_recv()
            for p in plane_order[:-1]:
                onward(apart, part, p).start()
    blocks = up_send.at[pl.ds(0, PLANE - 1)], up_send.at[pl.ds(0, PLANE)]
    for apart in (0, 1):
        all_of(HID_STRAIGHT + apart, blocks[apart]).wait_recv()
        for p in range(PLANE):
            if apart + p:
                part_down = part_down + down(peers[apart * PLANE + p])
    all_of(MIX, mix_all).wait_send()
    all_of(TO_RELAY, relay_recv).wait_send()
    all_of(STRAIGHT, up_recv.at[pl.ds(0, others - PLANE)]).wait_send()
    from_relay.wait_send()
    all_of(HID_LEVEL, up_send.at[pl.ds(0, 2)]).wait_send()
    all_of(HID_STRAIGHT, up_send.at[pl.ds(0, 2 * PLANE - 1)]).wait_send()
    for k in (8, 9, 10, 11, 12, 13, 14, 15):
        if k % PLANE:
            arrived(k).wait_recv()
        part_down = part_down + down(peers[k])
    send8[...] = part_down
    swap8 = remote(SWAP_TWO, SWAP_TWO, send8, recv8, me, far)
    swap8.start()
    all_of(HID_ON, up_send.at[pl.ds(0, 2 * PLANE - 2)]).wait_send()
    swap8.wait_recv()
    out[...] = (residual + (part_down + recv8[...])).astype(bf16)
    swap8.wait_send()


def fits(kv_n, tp_n, seqs, cols, heads, heads_all, pos_here, dim, units):
    if tp_n != 2 or kv_n != PLANE * PLANE or heads != 8 or seqs != 32:
        return False
    return (
        cols % LANES == 0 and pos_here == LANES and dim == LANES
        and heads_all == 2 * heads and units % (kv_n * LANES) == 0
    )


def layer(
    stream, gain_in, w_query, w_key, w_value, w_forget, keys_cache, values_cache,
    decay_cache, lengths, gain_att, w_out, gain_mlp, w_up, w_down,
):
    kv_n, tp_n = lax.axis_size("kv"), lax.axis_size("tp")
    seqs, cols = stream.shape
    heads, pos_here, dim = keys_cache.shape[1:]
    heads_all = w_forget.shape[1]
    units = w_up.shape[1]
    if not fits(kv_n, tp_n, seqs, cols, heads, heads_all, pos_here, dim, units):
        return per_device(
            stream, gain_in, w_query, w_key, w_value, w_forget, keys_cache, values_cache,
            decay_cache, lengths, gain_att, w_out, gain_mlp, w_up, w_down,
        )
    rows = seqs * heads // kv_n
    hidden_here = units // kv_n
    chunks = 4
    anywhere = pl.BlockSpec(memory_space=pl.ANY)

    def held(*shape, kind=bf16):
        return pltpu.VMEM(shape, kind)

    return pl.pallas_call(
        functools.partial(layer_kernel, kv_n),
        out_shape=pltpu.VMEM((seqs, cols), bf16),
        in_specs=[anywhere] * 15,
        out_specs=pl.BlockSpec(memory_space=pltpu.VMEM),
        scratch_shapes=[
            pltpu.SMEM((seqs,), jnp.int32),
            held(seqs, cols),
            held(cols),
            held(*gain_att.shape),
            held(cols),
            held(*decay_cache.shape, kind=f32),
            held(heads, cols),
            held(*w_query.shape),
            held(*w_key.shape),
            held(*w_value.shape),
            held(*keys_cache.shape),
            held(seqs, 2 * dim, heads // 2 * pos_here),
            held(*values_cache.shape),
            held(*w_out.shape),
            held(*w_up.shape),
            held(*w_down.shape),
            held(*gain_att.shape),
            held(kv_n, rows, dim),
            held(kv_n, rows, dim),
            held(heads, LANES, kind=f32),
            held(kv_n, LANES, kind=f32),
            held(kv_n, 2 * rows, dim),
            held(kv_n, 2 * rows, dim),
            held(rows, dim),
            held(kv_n, rows, dim),
            held(kv_n * rows, dim, kind=f32),
            held(kv_n * rows, dim, kind=f32),
            held(kv_n, rows, dim),
            held(kv_n, rows, dim),
            held(kv_n, LANES, kind=f32),
            held(kv_n, LANES, kind=f32),
            held(rows, dim),
            held(kv_n, rows, dim),
            held(8, LANES, kind=f32),
            held(kv_n, LANES, kind=f32),
            held(seqs, cols + LANES, kind=f32),
            held(seqs, cols + LANES, kind=f32),
            held(8, LANES, kind=f32),
            held(kv_n, LANES, kind=f32),
            held(kv_n, seqs, hidden_here),
            held(PLANE, seqs, hidden_here),
            held(seqs, hidden_here),
            held(kv_n - PLANE, seqs, hidden_here),
            held(kv_n, seqs, hidden_here),
            held(seqs, cols, kind=f32),
            held(seqs, cols, kind=f32),
            pltpu.SemaphoreType.DMA((13,)),
            pltpu.SemaphoreType.DMA((2, chunks)),
            pltpu.SemaphoreType.DMA((SENDS,)),
            pltpu.SemaphoreType.DMA((ARRIVALS,)),
        ],
        compiler_params=pltpu.CompilerParams(
            collective_id=0, has_side_effects=True, vmem_limit_bytes=60 * 1024 * 1024
        ),
    )(
        lengths, stream, gain_in, gain_att,
        gain_mlp, decay_cache,
        w_forget.T, w_query, w_key, w_value, keys_cache, values_cache, w_out, w_up, w_down,
    )


def solution(mesh):
    in_specs = (
        P(None, "kv"),
        P("kv"),
        P("kv", "tp"),
        P("kv", "tp"),
        P("kv", "tp"),
        P(),
        P(None, "tp", "kv", None),
        P(None, "tp", "kv", None),
        P(None, "tp", "kv"),
        P(),
        P("tp"),
        P("tp", "kv"),
        P("kv"),
        P("kv", "tp"),
        P("tp", "kv"),
    )
    out_specs = P(None, "kv")
    return jax.shard_map(
        layer, mesh=mesh, in_specs=in_specs, out_specs=out_specs, check_vma=False
    )
```

```python
import functools
import math

import jax
import jax.numpy as jnp
from jax import lax
from jax.experimental import pallas as pl
from jax.experimental.pallas import tpu as pltpu
from jax.sharding import PartitionSpec as P

f32 = jnp.float32
bf16 = jnp.bfloat16
LANES = 128
PLANE = 4

norm_eps = 1e-06
masked_score = -1e30


def merged_2(value, axis, join):
    pieces = jax.tree.map(lambda part: lax.all_gather(part, axis), value)
    head = jax.tree.map(lambda part: part[0], pieces)
    tail = jax.tree.map(lambda part: part[1:], pieces)
    so_far, _ = lax.scan(lambda so_far, share: (join(so_far, share), None), head, tail)
    return so_far


def fold_parts(left_part, right_part):
    peak_all = jnp.maximum(left_part[0], right_part[0])
    weight_one = jnp.exp(left_part[0] - peak_all)
    weight_two = jnp.exp(right_part[0] - peak_all)
    total_sum = left_part[1] * weight_one + right_part[1] * weight_two
    merged = left_part[2] * weight_one[..., None] + right_part[2] * weight_two[..., None]
    return (peak_all, total_sum, merged)


def per_device(
    stream,
    gain_in,
    w_query,
    w_key,
    w_value,
    w_forget,
    keys_cache,
    values_cache,
    decay_cache,
    lengths,
    gain_att,
    w_out,
    gain_mlp,
    w_up,
    w_down,
):
    kv_index = lax.axis_index("kv")
    tp_index = lax.axis_index("tp")
    kv_count = lax.axis_size("kv")
    seqs_here, cols_here = stream.shape
    heads_here = keys_cache.shape[1]
    pos_here = keys_cache.shape[2]
    head_dim = keys_cache.shape[3]
    width_all = cols_here * kv_count
    score_scale = 1.0 / math.sqrt(head_dim)
    stream_float = stream.astype(jnp.float32)
    scaled = (stream_float * gain_in.astype(jnp.float32)).astype(jnp.bfloat16)
    square_sum = jnp.sum(stream_float * stream_float, axis=1)
    forget_rows = lax.dynamic_slice(
        w_forget, (kv_index * cols_here, tp_index * heads_here), (cols_here, heads_here)
    )
    part_query = jnp.dot(scaled, w_query, preferred_element_type=jnp.float32)
    part_key = jnp.dot(scaled, w_key, preferred_element_type=jnp.float32)
    part_value = jnp.dot(scaled, w_value, preferred_element_type=jnp.float32)
    part_forget = jnp.dot(scaled, forget_rows, preferred_element_type=jnp.float32)
    part_query, part_key, part_value, part_forget, square_total = lax.psum(
        (part_query, part_key, part_value, part_forget, square_sum), "kv"
    )
    scale_in = lax.rsqrt(square_total / width_all + norm_eps)[:, None]
    queries = (part_query * scale_in).astype(jnp.bfloat16).reshape(seqs_here, heads_here, head_dim)
    key_new = (part_key * scale_in).astype(jnp.bfloat16).reshape(seqs_here, heads_here, head_dim)
    value_new = (
        (part_value * scale_in).astype(jnp.bfloat16).reshape(seqs_here, heads_here, head_dim)
    )
    forget = jax.nn.log_sigmoid(part_forget * scale_in)
    attention_logits = (
        jnp.einsum("shd,shpd->shp", queries, keys_cache, preferred_element_type=jnp.float32)
        * score_scale
    )
    attention_logits = attention_logits + forget[:, :, None] + decay_cache
    cache_positions = kv_index * pos_here + lax.iota(jnp.int32, pos_here)
    live_mask = (cache_positions[None, :] < lengths[:, None])[:, None, :]
    attention_logits = jnp.where(live_mask, attention_logits, masked_score)
    block_peak = jnp.max(attention_logits, axis=2)
    weights = jnp.where(live_mask, jnp.exp(attention_logits - block_peak[..., None]), 0.0)
    block_total = jnp.sum(weights, axis=2)
    block_out = jnp.einsum(
        "shp,shpd->shd",
        weights.astype(jnp.bfloat16),
        values_cache,
        preferred_element_type=jnp.float32,
    )
    peak_all, total_all, out_all = merged_2((block_peak, block_total, block_out), "kv", fold_parts)
    own_score = (
        jnp.sum(queries.astype(jnp.float32) * key_new.astype(jnp.float32), axis=2) * score_scale
    )
    top_score = jnp.maximum(peak_all, own_score)
    past_weight = jnp.exp(peak_all - top_score)
    own_weight = jnp.exp(own_score - top_score)
    numerator = (
        out_all * past_weight[..., None] + value_new.astype(jnp.float32) * own_weight[..., None]
    )
    denominator = total_all * past_weight + own_weight
    attended = (numerator / denominator[..., None]).reshape(seqs_here, heads_here * head_dim)
    attended_in = (attended * gain_att.astype(jnp.float32)).astype(jnp.bfloat16)
    part_out = jnp.dot(attended_in, w_out, preferred_element_type=jnp.float32)
    att_squares = jnp.sum(attended * attended, axis=1)
    part_out, att_total = lax.psum((part_out, att_squares), "tp")
    scale_att = lax.rsqrt(att_total / (attended.shape[1] * lax.axis_size("tp")) + norm_eps)[:, None]
    residual = (stream_float + scale_att * part_out).astype(jnp.bfloat16)
    residual_float = residual.astype(jnp.float32)
    mixer_in = (residual_float * gain_mlp.astype(jnp.float32)).astype(jnp.bfloat16)
    mixer_squares = jnp.sum(residual_float * residual_float, axis=1)
    part_up = jnp.dot(mixer_in, w_up, preferred_element_type=jnp.float32)
    pre_act, mixer_total = lax.psum((part_up, mixer_squares), "kv")
    scale_mixer = lax.rsqrt(mixer_total / width_all + norm_eps)[:, None]
    hidden = jnp.square(jax.nn.relu(pre_act * scale_mixer)).astype(jnp.bfloat16)
    part_down = jnp.dot(hidden, w_down, preferred_element_type=jnp.float32)
    mixer_out = lax.psum(part_down, "tp")
    return (residual_float + mixer_out).astype(jnp.bfloat16)


def lanes_of(shape):
    return lax.broadcasted_iota(jnp.int32, shape, 1)


def rows_of(shape):
    return lax.broadcasted_iota(jnp.int32, shape, 0)


def to_column(row, count, *starts):
    shape = (count, LANES)
    apart = lanes_of(shape) - rows_of(shape)
    hit = functools.reduce(jnp.logical_or, [apart == start for start in starts])
    return jnp.sum(
        jnp.where(hit, jnp.broadcast_to(row, shape), 0.0), axis=1, keepdims=True
    )


def to_row(column, start):
    shape = (column.shape[0], LANES)
    hit = lanes_of(shape) - rows_of(shape) == start
    return jnp.sum(
        jnp.where(hit, jnp.broadcast_to(column, shape), 0.0), axis=0, keepdims=True
    )


Q, STAT, KV, Q_ALL, OUT, PEAK, ATT, SQUARE, MIX, GAIN, SWAP_ONE, SWAP_TWO = range(12)
TO_RELAY, STRAIGHT, FROM_RELAY, HID_STRAIGHT, HID_LEVEL, HID_ON = 12, 13, 14, 15, 17, 21
SENDS, ARRIVALS, STRAIGHT_OWN = 22, 30, 29


def layer_kernel(
    kv_n,
    lengths, stream, gain_in, gain_att, gain_mlp, decay,
    w_forget, w_query, w_key, w_value, keys, values, w_out, w_up, w_down,
    out,
    len_s, x_v, gi_v, ga_v, gm_v, decay_v,
    wf_v, wq_v, wk_v, wv_v, keys_v, keys_turned, values_v, wo_v, wu_v, wd_v,
    gain_far, q_send, q_recv, st_send, st_recv, kv_send, kv_recv,
    q_own, q_all, q_float, o_float, o_send, o_recv, pk_send, pk_recv,
    att_own, att_all, sq_own, sq_all, send5, recv5,
    mix_own, mix_all, up_send, relay_recv, relay_send, up_recv,
    hid_all, send8, recv8,
    load_sem, cache_sem, ssem, rsem,
):
    me = lax.axis_index("kv")
    tp = lax.axis_index("tp")
    far = 1 - tp
    seqs, cols = x_v.shape
    heads = decay_v.shape[1]
    pos_here = decay_v.shape[2]
    dim = keys_v.shape[-1]
    rows = q_own.shape[0]
    groups = seqs // rows
    hidden_here = hid_all.shape[2]
    chunks = cache_sem.shape[1]
    per_chunk = seqs // chunks
    width_all = cols * kv_n
    others = kv_n - 1
    score_scale = 1.0 / math.sqrt(dim)
    together = math.gcd(8, per_chunk)

    level, spot = me // PLANE, me % PLANE
    levels = (level, level + 1 - 2 * (level % 2), (level + 2) % 4, 3 - level)
    side, along = spot // 2, spot % 2
    spots = (
        spot, side * 2 + 1 - along, (1 - side) * 2 + along, (1 - side) * 2 + 1 - along
    )
    peers = [levels[k // PLANE] * PLANE + spots[k % PLANE] for k in range(kv_n)]
    far_first = (15, 14, 13, 11, 12, 10, 9, 7, 8, 6, 5, 3, 4, 2, 1, 0)
    plane_order = (3, 1, 2, 0)
    my_group, my_head = me // heads, me % heads

    barrier = pltpu.get_barrier_semaphore()
    for k in far_first:
        pl.semaphore_signal(
            barrier, inc=1, device_id=(peers[k], far), device_id_type=pl.DeviceIdType.MESH
        )

    def load(src, dst, index):
        return pltpu.make_async_copy(src, dst, load_sem.at[index])

    start_row = pl.multiple_of(me * cols, cols)
    first_head = pl.multiple_of(tp * heads, heads)
    first_loads = [
        load(stream, x_v, 0),
        load(gain_in, gi_v, 1),
        load(w_query, wq_v, 2),
        load(w_forget.at[pl.ds(first_head, heads), pl.ds(start_row, cols)], wf_v, 3),
        load(w_key, wk_v, 4),
        load(w_value, wv_v, 5),
    ]
    small_loads = [
        load(gain_att, ga_v, 6), load(decay, decay_v, 7), load(lengths, len_s, 8),
        load(gain_mlp, gm_v, 9),
    ]
    late_loads = [load(w_out, wo_v, 10), load(w_up, wu_v, 11), load(w_down, wd_v, 12)]
    for copy in first_loads:
        copy.start()
    for copy in small_loads:
        copy.start()

    def cache_copy(which, chunk):
        src, dst = ((keys, keys_v), (values, values_v))[which]
        part = pl.ds(chunk * per_chunk, per_chunk)
        return pltpu.make_async_copy(src.at[part], dst.at[part], cache_sem.at[which, chunk])

    def remote(sent, landed, src, dst, device, core):
        return pltpu.make_async_remote_copy(
            src_ref=src, dst_ref=dst, send_sem=ssem.at[sent], recv_sem=rsem.at[landed],
            device_id=(device, core), device_id_type=pl.DeviceIdType.MESH,
        )

    def all_of(index, held):
        return remote(index, index, held, held, me, far)

    def scatter(phase, send, recv, k):
        remote(phase, phase, send.at[peers[k]], recv.at[k], peers[k], far).start()

    def row_to(phase, src, recv, k):
        remote(phase, phase, src, recv.at[pl.ds(k, 1)], peers[k], far).start()

    def spread(phase, own, held, k):
        remote(phase, phase, own, held.at[me], peers[k], far).start()

    for copy in first_loads[:4]:
        copy.wait()
    x = x_v[...].astype(f32)
    scaled = (x * gi_v[...].astype(f32).reshape(1, -1)).astype(bf16)

    def by_owner(dst, part, place):
        for g in range(groups):
            for h in range(heads):
                dst[g * heads + h, place * rows:(place + 1) * rows, :] = part[
                    g * rows:(g + 1) * rows, h * dim:(h + 1) * dim
                ]

    by_owner(q_send, jnp.dot(scaled, wq_v[...], preferred_element_type=f32).astype(bf16), 0)
    squares = x * x
    high = squares.astype(bf16)
    low = (squares - high.astype(f32)).astype(bf16)
    blank = jnp.zeros((32, cols), bf16)
    last = (((1,), (1,)), ((), ()))
    st_send[...] = lax.dot_general(
        jnp.ones((heads, cols), bf16), jnp.concatenate([high, blank, low, blank], axis=0),
        last, preferred_element_type=f32,
    ) + lax.dot_general(
        wf_v[...], jnp.concatenate([blank, scaled, blank, blank], axis=0),
        last, preferred_element_type=f32,
    )
    for copy in first_loads[4:]:
        copy.wait()
    for copy in small_loads:
        copy.wait()
    for chunk in range(chunks):
        cache_copy(0, chunk).start()
    for chunk in range(chunks):
        cache_copy(1, chunk).start()
    for copy in late_loads:
        copy.start()
    pl.semaphore_wait(barrier, kv_n)
    for k in far_first:
        scatter(Q, q_send, q_recv, k)
        row_to(STAT, st_send.at[pl.ds(peers[k] % heads, 1)], st_recv, k)
    gain_swap = remote(GAIN, GAIN, ga_v, gain_far, me, far)
    gain_swap.start()
    for place, weight in enumerate((wk_v, wv_v)):
        by_owner(
            kv_send, jnp.dot(scaled, weight[...], preferred_element_type=f32).astype(bf16), place
        )
    total = jnp.zeros((rows, dim), f32)

    def turn_chunk(chunk, carry):
        cache_copy(0, chunk).wait()

        def turn(i, c):
            s = chunk * per_chunk + i
            for h in range(heads):
                keys_turned[
                    s, h % 2 * dim:(h % 2 + 1) * dim, h // 2 * pos_here:(h // 2 + 1) * pos_here
                ] = keys_v[s, h].T
            return c

        return lax.fori_loop(0, per_chunk, turn, carry)

    lax.fori_loop(0, chunks // 2, turn_chunk, 0)
    all_of(STAT, st_recv).wait_recv()
    all_of(Q, q_recv).wait_recv()
    for k in range(kv_n):
        total = total + q_recv[k].astype(f32)
    stat_row = jnp.sum(st_recv[...], axis=0, keepdims=True)
    first_lane = my_group * rows
    scale_in = lax.rsqrt(
        to_column(stat_row, rows, first_lane, first_lane + 64) / width_all + norm_eps
    )
    query = (total * scale_in).astype(bf16)
    q_own[...] = query
    for k in far_first:
        spread(Q_ALL, q_own, q_all, k)
    for k in far_first:
        scatter(KV, kv_send, kv_recv, k)
    gate = to_column(stat_row, rows, first_lane + 32) * scale_in
    forget = jnp.minimum(gate, 0.0) - jnp.log1p(jnp.exp(-jnp.abs(gate)))

    lax.fori_loop(chunks // 2, chunks, turn_chunk, 0)
    all_of(Q_ALL, q_all).wait_recv()
    q_float[...] = q_all[...].reshape(kv_n * rows, dim).astype(f32)
    head_row = rows_of((heads, pos_here))
    position = me * pos_here + lanes_of((heads, pos_here))
    lane_h = lanes_of((heads, LANES))

    even = rows_of((heads, dim)) % 2 == 0

    def in_pairs(cache, s):
        return jnp.concatenate(
            [
                jnp.concatenate([cache[s, h], cache[s, h + 1]], axis=1)
                for h in range(0, heads, 2)
            ],
            axis=0,
        )

    def some_sequences(first_seq, marks):
        batch = [first_seq + i for i in range(together)]
        places = [
            pl.ds((s // rows) * (heads * rows) + s % rows, heads, stride=rows) for s in batch
        ]
        q_parts = [q_float[mine, :] for mine in places]
        everies = [
            lax.dot_general(
                jnp.concatenate(
                    [jnp.where(even, q_s, 0.0), jnp.where(even, 0.0, q_s)], axis=1
                ).astype(bf16),
                keys_turned[s], (((1,), (0,)), ((), ())), preferred_element_type=f32,
            )
            for q_s, s in zip(q_parts, batch)
        ]
        spreads = []
        for every, s in zip(everies, batch):
            score = every[:, :pos_here]
            for pair in range(1, heads // 2):
                score = jnp.where(
                    head_row // 2 == pair, every[:, pair * pos_here:(pair + 1) * pos_here], score
                )
            score = score * score_scale + decay_v[s]
            live = position < len_s[s]
            score = jnp.where(live, score, masked_score)
            peak = jnp.max(score, axis=1, keepdims=True)
            probs = jnp.where(live, jnp.exp(score - peak), 0.0)
            block_total = jnp.sum(probs, axis=1, keepdims=True)
            spreads.append(jnp.concatenate(
                [jnp.where(head_row // 2 == pair, probs, 0.0) for pair in range(heads // 2)],
                axis=1,
            ).astype(bf16))
            marks = jnp.where(lane_h == s % rows, peak, marks)
            marks = jnp.where(lane_h == s % rows + rows, block_total, marks)
        outs = [
            jnp.dot(part, in_pairs(values_v, s), preferred_element_type=f32)
            for part, s in zip(spreads, batch)
        ]
        for mine, out_s in zip(places, outs):
            o_float[mine, :] = jnp.where(even, out_s[:, :dim], out_s[:, dim:])
        return marks

    def one_chunk(chunk, marks):
        cache_copy(1, chunk).wait()

        def inner(i, c):
            return some_sequences(chunk * per_chunk + together * i, c)

        return lax.fori_loop(0, per_chunk // together, inner, marks)

    group_chunks = chunks // groups
    for g in range(groups):
        marks = lax.fori_loop(
            g * group_chunks, (g + 1) * group_chunks, one_chunk, jnp.zeros((heads, LANES), f32)
        )
        mine = slice(g * heads, (g + 1) * heads)
        pk_send[mine, :] = marks
        o_send[mine] = o_float[g * heads * rows:(g + 1) * heads * rows, :].astype(bf16).reshape(
            heads, rows, dim
        )
        for step in (1, 0):
            for p in plane_order:
                owner = (g * 2 + (level + step) % 2) * PLANE + spots[p]
                remote(OUT, OUT, o_send.at[owner], o_recv.at[me], owner, far).start()
                remote(
                    PEAK, PEAK, pk_send.at[pl.ds(owner, 1)], pk_recv.at[pl.ds(me, 1)], owner, far
                ).start()

    keys_total = jnp.zeros((2 * rows, dim), f32)
    all_of(KV, kv_recv).wait_recv()
    for k in range(kv_n):
        keys_total = keys_total + kv_recv[k].astype(f32)
    key_new = (keys_total[:rows] * scale_in).astype(bf16).astype(f32)
    value_new = (keys_total[rows:] * scale_in).astype(bf16).astype(f32)
    own_score = jnp.sum(query.astype(f32) * key_new, axis=1, keepdims=True) * score_scale
    gain_swap.wait_recv()
    gain_here = gain_far[...].astype(f32).reshape(1, -1)
    gain_head = gain_here[:, :dim]
    for h in range(1, heads):
        gain_head = jnp.where(my_head == h, gain_here[:, h * dim:(h + 1) * dim], gain_head)

    for copy in late_loads:
        copy.wait()
    for index, held in ((Q, q_recv), (STAT, st_recv), (KV, kv_recv), (Q_ALL, q_all)):
        all_of(index, held).wait_send()
    gain_swap.wait_send()
    all_of(PEAK, pk_recv).wait_recv()
    peaks = pk_recv[...]
    top_row = jnp.max(peaks, axis=0, keepdims=True)
    shares = jnp.exp(peaks - top_row)
    total_row = jnp.sum(shares * pltpu.roll(peaks, LANES - rows, 1), axis=0, keepdims=True)
    peak_all = to_column(top_row, rows, 0) + forget
    total_all = to_column(total_row, rows, 0)
    share_columns = [to_column(shares[k:k + 1], rows, 0) for k in range(kv_n)]
    top = jnp.maximum(peak_all, own_score)
    past_weight = jnp.exp(peak_all - top)
    own_weight = jnp.exp(own_score - top)
    out_all = jnp.zeros((rows, dim), f32)
    all_of(OUT, o_recv).wait_recv()
    for k in range(kv_n):
        out_all = out_all + share_columns[k] * o_recv[k].astype(f32)
    attended_one = (out_all * past_weight + value_new * own_weight) / (
        total_all * past_weight + own_weight
    )
    att_own[...] = (attended_one * gain_head).astype(bf16)
    squares_one = jnp.sum(attended_one * attended_one, axis=1, keepdims=True)
    sq_own[...] = jnp.broadcast_to(to_row(squares_one, first_lane), sq_own.shape)
    for k in far_first:
        spread(ATT, att_own, att_all, k)
        row_to(SQUARE, sq_own.at[pl.ds(0, 1)], sq_all, k)

    all_of(ATT, att_all).wait_recv()
    all_of(SQUARE, sq_all).wait_recv()
    attended_in = jnp.concatenate(
        [
            jnp.concatenate([att_all[g * heads + h] for g in range(groups)], axis=0)
            for h in range(heads)
        ],
        axis=1,
    )
    part_out = jnp.dot(attended_in, wo_v[...], preferred_element_type=f32)
    att_squares = to_column(jnp.sum(sq_all[...], axis=0, keepdims=True), seqs, 0)
    send5[:, :cols] = part_out
    send5[:, cols:] = jnp.broadcast_to(att_squares, (seqs, LANES))
    swap5 = remote(SWAP_ONE, SWAP_ONE, send5, recv5, me, far)
    swap5.start()
    swap5.wait_recv()
    width_att = attended_in.shape[1] * 2
    scale_att = lax.rsqrt((att_squares + recv5[:, cols:cols + 1]) / width_att + norm_eps)
    residual = (
        x_v[...].astype(f32) + scale_att * (part_out + recv5[:, :cols])
    ).astype(bf16).astype(f32)
    mixer_in = (residual * gm_v[...].astype(f32).reshape(1, -1)).astype(bf16)
    mixer_squares = jnp.sum(residual * residual, axis=1, keepdims=True)

    def up(apart):
        width = PLANE * hidden_here
        columns = pl.ds(pl.multiple_of(levels[apart] * width, LANES), width)
        return jnp.dot(mixer_in, wu_v[:, columns], preferred_element_type=f32)

    def store_up(apart):
        part = up(apart).astype(bf16)
        for place in range(PLANE):
            up_send[apart * PLANE + place] = part[
                :, place * hidden_here:(place + 1) * hidden_here
            ]

    def to_relay(p):
        return remote(
            TO_RELAY, TO_RELAY, up_send.at[2 * PLANE + spots[p]], relay_recv.at[p], peers[p], far
        )

    from_relay = remote(
        FROM_RELAY, FROM_RELAY, relay_send, up_recv.at[others - PLANE], peers[2 * PLANE], far
    )

    def straight(k):
        apart, p = k // PLANE, k % PLANE
        slot = k - 1 if k < 2 * PLANE else k - 1 - PLANE
        return remote(
            STRAIGHT, STRAIGHT_OWN if k < PLANE else STRAIGHT,
            up_send.at[apart * PLANE + spots[p]], up_recv.at[slot],
            peers[k], tp,
        )

    store_up(2)
    for p in plane_order:
        to_relay(p).start()
    store_up(3)
    for p in plane_order:
        straight(3 * PLANE + p).start()
    mix_own[...] = jnp.broadcast_to(to_row(mixer_squares, 0), mix_own.shape)
    for k in far_first:
        row_to(MIX, mix_own.at[pl.ds(0, 1)], mix_all, k)
    store_up(1)
    for p in plane_order:
        straight(PLANE + p).start()
    store_up(0)
    for p in plane_order[:-1]:
        straight(p).start()
    pre_act = up_send[spot].astype(f32)
    all_of(TO_RELAY, relay_recv).wait_recv()
    relayed = relay_recv[0].astype(f32)
    for p in range(1, PLANE):
        relayed = relayed + relay_recv[p].astype(f32)
    relay_send[...] = relayed.astype(bf16)
    from_relay.start()
    for index, held in ((OUT, o_recv), (PEAK, pk_recv), (ATT, att_all), (SQUARE, sq_all)):
        all_of(index, held).wait_send()
    swap5.wait_send()
    all_of(MIX, mix_all).wait_recv()
    mixer_total = to_column(jnp.sum(mix_all[...], axis=0, keepdims=True), seqs, 0)
    scale_mixer = lax.rsqrt(mixer_total / width_all + norm_eps)
    remote(
        STRAIGHT, STRAIGHT, up_send.at[pl.ds(0, 2 * PLANE)], up_send.at[pl.ds(0, 2 * PLANE)], me, far
    ).wait_recv()
    for slot in range(PLANE - 1, others - PLANE):
        pre_act = pre_act + up_recv[slot].astype(f32)
    from_relay.wait_recv()
    pre_act = pre_act + up_recv[others - PLANE].astype(f32)
    all_of(STRAIGHT_OWN, up_send.at[pl.ds(0, PLANE - 1)]).wait_recv()
    for slot in range(PLANE - 1):
        pre_act = pre_act + up_recv[slot].astype(f32)
    hidden = jnp.maximum(pre_act * scale_mixer, 0.0)
    hid_all[me] = (hidden * hidden).astype(bf16)

    half = seqs // 2

    def to_level(apart, part):
        some = pl.ds(part * half, half)
        return remote(
            HID_LEVEL, HID_LEVEL + 2 * (apart - 2) + part, hid_all.at[me, some],
            hid_all.at[me, some], peers[apart * PLANE], tp,
        )

    def onward(apart, part, p):
        some = pl.ds(part * half, half)
        return remote(
            HID_ON, HID_ON + (apart - 2) * PLANE + p, hid_all.at[peers[apart * PLANE], some],
            hid_all.at[peers[apart * PLANE], some], peers[p], tp,
        )

    def arrived(k):
        index = HID_ON + k - 2 * PLANE
        return remote(index, index, hid_all.at[me], hid_all.at[peers[k]], peers[k], tp)

    for part in (0, 1):
        for apart in (2, 3):
            to_level(apart, part).start()
    for apart in (0, 1):
        for p in plane_order:
            k = apart * PLANE + p
            if k:
                remote(
                    HID_STRAIGHT, HID_STRAIGHT + apart, hid_all.at[me], hid_all.at[me],
                    peers[k], tp,
                ).start()

    def down(owner):
        depth = pl.ds(pl.multiple_of(owner * hidden_here, LANES), hidden_here)
        return jnp.dot(hid_all[owner], wd_v[depth, :], preferred_element_type=f32)

    part_down = down(me)
    for part in (0, 1):
        for apart in (2, 3):
            to_level(apart, part).wait_recv()
            for p in plane_order[:-1]:
                onward(apart, part, p).start()
    blocks = up_send.at[pl.ds(0, PLANE - 1)], up_send.at[pl.ds(0, PLANE)]
    for apart in (0, 1):
        all_of(HID_STRAIGHT + apart, blocks[apart]).wait_recv()
        for p in range(PLANE):
            if apart + p:
                part_down = part_down + down(peers[apart * PLANE + p])
    all_of(MIX, mix_all).wait_send()
    all_of(TO_RELAY, relay_recv).wait_send()
    all_of(STRAIGHT, up_recv.at[pl.ds(0, others - PLANE)]).wait_send()
    from_relay.wait_send()
    all_of(HID_LEVEL, up_send.at[pl.ds(0, 2)]).wait_send()
    all_of(HID_STRAIGHT, up_send.at[pl.ds(0, 2 * PLANE - 1)]).wait_send()
    for k in (8, 9, 10, 11, 12, 13, 14, 15):
        if k % PLANE:
            arrived(k).wait_recv()
        part_down = part_down + down(peers[k])
    send8[...] = part_down
    swap8 = remote(SWAP_TWO, SWAP_TWO, send8, recv8, me, far)
    swap8.start()
    all_of(HID_ON, up_send.at[pl.ds(0, 2 * PLANE - 2)]).wait_send()
    swap8.wait_recv()
    out[...] = (residual + (part_down + recv8[...])).astype(bf16)
    swap8.wait_send()


def fits(kv_n, tp_n, seqs, cols, heads, heads_all, pos_here, dim, units):
    if tp_n != 2 or kv_n != PLANE * PLANE or heads != 8 or seqs != 32:
        return False
    return (
        cols % LANES == 0 and pos_here == LANES and dim == LANES
        and heads_all == 2 * heads and units % (kv_n * LANES) == 0
    )


def layer(
    stream, gain_in, w_query, w_key, w_value, w_forget, keys_cache, values_cache,
    decay_cache, lengths, gain_att, w_out, gain_mlp, w_up, w_down,
):
    kv_n, tp_n = lax.axis_size("kv"), lax.axis_size("tp")
    seqs, cols = stream.shape
    heads, pos_here, dim = keys_cache.shape[1:]
    heads_all = w_forget.shape[1]
    units = w_up.shape[1]
    if not fits(kv_n, tp_n, seqs, cols, heads, heads_all, pos_here, dim, units):
        return per_device(
            stream, gain_in, w_query, w_key, w_value, w_forget, keys_cache, values_cache,
            decay_cache, lengths, gain_att, w_out, gain_mlp, w_up, w_down,
        )
    rows = seqs * heads // kv_n
    hidden_here = units // kv_n
    chunks = 2
    anywhere = pl.BlockSpec(memory_space=pl.ANY)

    def held(*shape, kind=bf16):
        return pltpu.VMEM(shape, kind)

    return pl.pallas_call(
        functools.partial(layer_kernel, kv_n),
        out_shape=pltpu.VMEM((seqs, cols), bf16),
        in_specs=[anywhere] * 15,
        out_specs=pl.BlockSpec(memory_space=pltpu.VMEM),
        scratch_shapes=[
            pltpu.SMEM((seqs,), jnp.int32),
            held(seqs, cols),
            held(cols),
            held(*gain_att.shape),
            held(cols),
            held(*decay_cache.shape, kind=f32),
            held(heads, cols),
            held(*w_query.shape),
            held(*w_key.shape),
            held(*w_value.shape),
            held(*keys_cache.shape),
            held(seqs, 2 * dim, heads // 2 * pos_here),
            held(*values_cache.shape),
            held(*w_out.shape),
            held(*w_up.shape),
            held(*w_down.shape),
            held(*gain_att.shape),
            held(kv_n, rows, dim),
            held(kv_n, rows, dim),
            held(heads, LANES, kind=f32),
            held(kv_n, LANES, kind=f32),
            held(kv_n, 2 * rows, dim),
            held(kv_n, 2 * rows, dim),
            held(rows, dim),
            held(kv_n, rows, dim),
            held(kv_n * rows, dim, kind=f32),
            held(kv_n * rows, dim, kind=f32),
            held(kv_n, rows, dim),
            held(kv_n, rows, dim),
            held(kv_n, LANES, kind=f32),
            held(kv_n, LANES, kind=f32),
            held(rows, dim),
            held(kv_n, rows, dim),
            held(8, LANES, kind=f32),
            held(kv_n, LANES, kind=f32),
            held(seqs, cols + LANES, kind=f32),
            held(seqs, cols + LANES, kind=f32),
            held(8, LANES, kind=f32),
            held(kv_n, LANES, kind=f32),
            held(kv_n, seqs, hidden_here),
            held(PLANE, seqs, hidden_here),
            held(seqs, hidden_here),
            held(kv_n - PLANE, seqs, hidden_here),
            held(kv_n, seqs, hidden_here),
            held(seqs, cols, kind=f32),
            held(seqs, cols, kind=f32),
            pltpu.SemaphoreType.DMA((13,)),
            pltpu.SemaphoreType.DMA((2, chunks)),
            pltpu.SemaphoreType.DMA((SENDS,)),
            pltpu.SemaphoreType.DMA((ARRIVALS,)),
        ],
        compiler_params=pltpu.CompilerParams(
            collective_id=0, has_side_effects=True, vmem_limit_bytes=60 * 1024 * 1024
        ),
    )(
        lengths, stream, gain_in, gain_att,
        gain_mlp, decay_cache,
        w_forget.T, w_query, w_key, w_value, keys_cache, values_cache, w_out, w_up, w_down,
    )


def solution(mesh):
    in_specs = (
        P(None, "kv"),
        P("kv"),
        P("kv", "tp"),
        P("kv", "tp"),
        P("kv", "tp"),
        P(),
        P(None, "tp", "kv", None),
        P(None, "tp", "kv", None),
        P(None, "tp", "kv"),
        P(),
        P("tp"),
        P("tp", "kv"),
        P("kv"),
        P("kv", "tp"),
        P("tp", "kv"),
    )
    out_specs = P(None, "kv")
    return jax.shard_map(
        layer, mesh=mesh, in_specs=in_specs, out_specs=out_specs, check_vma=False
    )
```
